512 devices in a mesh: sp: 256 (over z, y, x), tp: 2 (over core).
Axes of the slice: x: 4, y: 4, z: 16, core: 2. Of those that a mesh axis runs over, the one named last changes fastest.
Arguments:
- residual: bfloat16 [49152, 1024], P('sp', 'tp'), may hold values from -6 to 6
- query_first: bfloat16 [49152, 1024], P('sp', 'tp'), may hold values from -64 to 64
- key_first: bfloat16 [49152, 256], P('sp', 'tp'), may hold values from -20 to 20
- value_first: bfloat16 [49152, 256], P('sp', 'tp'), may hold values from -6 to 6
- documents: int32 [49152], P('sp'), may hold values from 0 to 53, as said below
- bias_first: float32 [16, 513], P('tp'), may hold values from -4 to 4
- out_first: bfloat16 [1024, 1024], P('tp'), may hold values from -0.75 to 0.75
- norm_gain: float32 [1024], replicated, may hold values from 0.1 to 1.9
- query_w: bfloat16 [1024, 1024], P(None, 'tp'), may hold values from -0.1875 to 0.1875
- key_w: bfloat16 [1024, 256], P(None, 'tp'), may hold values from -0.1875 to 0.1875
- value_w: bfloat16 [1024, 256], P(None, 'tp'), may hold values from -0.1875 to 0.1875
- bias_second: float32 [16, 513], P('tp'), may hold values from -4 to 4
- out_second: bfloat16 [1024, 1024], P('tp'), may hold values from -0.75 to 0.75
Outputs:
- layer_two: bfloat16 [49152, 1024], P('sp', 'tp')
The draws below stay inside these ranges and needn't reach their ends.
Inputs may be any that keep to these rules, and one draw needn't show every extreme that they name: Document numbers start at 0, never fall, and rise by one at the first position of each document; there are exactly 54 documents, each of at least 896 positions.
All inputs are finite; a program needn't handle non-finite values.
Results may differ from the reference program's by a relative error of at most 0.017.
Values may be sent and summed in bfloat16 or wider, within the bound.
No kernel may reach another device: no remote copies, remote signals or barrier semaphores. Data moves between devices by JAX's collectives and lax.ppermute only.
A program may use at most 64 MiB of HBM per device.

```python
import jax
import jax.numpy as jnp
from jax import lax

D = 1024
HEADS = 16
KV_HEADS = 4
HEAD_SIZE = 64
SEG = 64
PAST = 4
REL_CLIP = 256
TOKENS = 49152
DOC_MIN = 896
N_TP = 2


def paired_draw(key):
    base = jax.random.fold_in(key, 11)
    key_noise, query_noise = jax.random.split(base, 2)
    keys_raw = jnp.clip(jax.random.normal(key_noise, (TOKENS, KV_HEADS, HEAD_SIZE), jnp.float32), -4.0, 4.0)
    queries_raw = jnp.clip(jax.random.normal(query_noise, (TOKENS, KV_HEADS, HEADS // KV_HEADS, HEAD_SIZE), jnp.float32), -4.0, 4.0)
    keys_new = keys_raw
    queries_new = queries_raw
    return (queries_new.reshape(TOKENS, HEADS * HEAD_SIZE), keys_new.reshape(TOKENS, KV_HEADS * HEAD_SIZE))


def draw_query_first(key, part):
    return paired_draw(key)[0].astype(jnp.bfloat16)


def draw_key_first(key, part):
    return paired_draw(key)[1].astype(jnp.bfloat16)


def draw_documents(key, part):
    doc_count = TOKENS // DOC_MIN
    spare_rows = TOKENS - doc_count * DOC_MIN
    base = jax.random.fold_in(key, 23)
    cut_points = jnp.sort(jax.random.randint(base, (doc_count,), 0, spare_rows + 1))
    starts = jnp.arange(doc_count) * DOC_MIN + cut_points
    positions = jnp.arange(TOKENS)
    counted = (starts[None, 1:] <= positions[:, None]).astype(jnp.int32)
    return jnp.sum(counted, axis=1).astype(jnp.int32)


def levels(own_key, dims, shards, least, high):
    def one(dim, parts):
        draws = jax.random.uniform(jax.random.fold_in(jax.random.fold_in(own_key, 6), dim), (parts,), jnp.float32, least / len(shards), high / len(shards))
        return jnp.repeat(jnp.exp(draws), dims[dim] // parts).reshape((-1,) + (1,) * (len(dims) - dim - 1))

    loudness = one(*shards[0])
    for cut in shards[1:]:
        loudness = loudness * one(*cut)
    return loudness


def normal_values(own_key, shape, scale, most, shards=(), kind=jnp.bfloat16):
    drawn = scale * jax.random.normal(own_key, shape, jnp.float32)
    if shards:
        drawn = drawn * levels(own_key, shape, shards, -0.22, 0.18)
    return jnp.clip(drawn, -most, most).astype(kind)


def setup_inputs(seed: int = 0) -> dict:
    streams_of = jax.random.split(jax.random.key(seed), 14)
    residual = normal_values(streams_of[0], (TOKENS, D), 1.0, 6.0, ((0, 256), (1, 2)))
    query_first = draw_query_first(jax.random.fold_in(streams_of[13], 71), 0)
    key_first = draw_key_first(jax.random.fold_in(streams_of[13], 71), 0)
    value_first = normal_values(streams_of[3], (TOKENS, KV_HEADS * HEAD_SIZE), 1.0, 6.0, ((0, 256), (1, 2)))
    documents = draw_documents(jax.random.fold_in(streams_of[13], 71), 0)
    bias_first = normal_values(streams_of[5], (HEADS, 2 * REL_CLIP + 1), 1.0, 4.0, ((0, 2),), jnp.float32)
    out_first = normal_values(streams_of[6], (HEADS * HEAD_SIZE, D), (HEADS * HEAD_SIZE // 16) ** -0.5, 0.75, ((0, 2),))
    norm_gain = jnp.clip(1.0 + 0.18 * jax.random.normal(streams_of[7], (D,), jnp.float32), 0.1, 1.9)
    query_w = normal_values(streams_of[8], (D, HEADS * HEAD_SIZE), D ** -0.5, 0.1875, ((1, 2),))
    key_w = normal_values(streams_of[9], (D, KV_HEADS * HEAD_SIZE), D ** -0.5, 0.1875, ((1, 2),))
    value_w = normal_values(streams_of[10], (D, KV_HEADS * HEAD_SIZE), D ** -0.5, 0.1875, ((1, 2),))
    bias_second = normal_values(streams_of[11], (HEADS, 2 * REL_CLIP + 1), 1.0, 4.0, ((0, 2),), jnp.float32)
    out_second = normal_values(streams_of[12], (HEADS * HEAD_SIZE, D), (HEADS * HEAD_SIZE // 16) ** -0.5, 0.75, ((0, 2),))
    return dict(residual=residual, query_first=query_first, key_first=key_first, value_first=value_first, documents=documents, bias_first=bias_first, out_first=out_first, norm_gain=norm_gain, query_w=query_w, key_w=key_w, value_w=value_w, bias_second=bias_second, out_second=out_second)


eps = 1e-06

def segment_attention(queries, keys, values, documents, bias_table):
    total_rows = queries.shape[0]
    span_rows = PAST * SEG
    band_rows = span_rows + SEG
    group_size = HEADS // KV_HEADS
    keys_pad = jnp.concatenate([jnp.zeros((span_rows, keys.shape[1]), keys.dtype), keys], axis=0)
    values_pad = jnp.concatenate([jnp.zeros((span_rows, values.shape[1]), values.dtype), values], axis=0)
    docs_pad = jnp.concatenate([jnp.full((span_rows,), -1, jnp.int32), documents.astype(jnp.int32)], axis=0)
    query_pos = jnp.arange(SEG, dtype=jnp.int32)[:, None]
    key_pos = jnp.arange(band_rows, dtype=jnp.int32)[None, :]
    relative = jnp.clip(query_pos + span_rows - key_pos, -REL_CLIP, REL_CLIP) + REL_CLIP
    position_bias_grid = jnp.take(bias_table.astype(jnp.float32), relative, axis=1).reshape(KV_HEADS, group_size, SEG, band_rows)
    seg_count = total_rows // SEG

    def one_segment(segment):
        first_row = (segment * SEG).astype(jnp.int32)
        query_tile_rows = lax.dynamic_slice_in_dim(queries, first_row, SEG, 0).astype(jnp.float32).reshape(SEG, KV_HEADS, group_size, HEAD_SIZE)
        key_tile_rows = lax.dynamic_slice_in_dim(keys_pad, first_row, band_rows, 0).astype(jnp.float32).reshape(band_rows, KV_HEADS, HEAD_SIZE)
        value_tile_rows = lax.dynamic_slice_in_dim(values_pad, first_row, band_rows, 0).astype(jnp.float32).reshape(band_rows, KV_HEADS, HEAD_SIZE)
        band_docs = lax.dynamic_slice_in_dim(docs_pad, first_row, band_rows, 0)
        own_docs = lax.dynamic_slice_in_dim(documents.astype(jnp.int32), first_row, SEG, 0)
        logit_scores = jnp.einsum('yixw,ziw->ixyz', query_tile_rows, key_tile_rows) * HEAD_SIZE ** (-0.5) + position_bias_grid
        allowed = band_docs[None, :] == own_docs[:, None]
        logit_scores = jnp.where(allowed[None, None], logit_scores, -jnp.inf)
        largest = lax.optimization_barrier(jnp.max(logit_scores, axis=-1, keepdims=True))
        softmax_weight = jnp.exp(logit_scores - largest)
        softmax_weight = (softmax_weight / lax.optimization_barrier(jnp.sum(softmax_weight, axis=-1, keepdims=True))).astype(jnp.bfloat16)
        blended_output = jnp.einsum('rsvh,hru->vrsu', softmax_weight.astype(jnp.float32), value_tile_rows)
        return blended_output.astype(jnp.bfloat16).reshape(SEG, HEADS * HEAD_SIZE)
    blocks = lax.map(one_segment, jnp.arange(seg_count, dtype=jnp.int32))
    return blocks.reshape(total_rows, HEADS * HEAD_SIZE)

def project_out(mixed, weight):
    share_width = mixed.shape[1] // N_TP
    total_sum = jnp.zeros((mixed.shape[0], weight.shape[1]), jnp.float32)
    for group_index in range(N_TP):
        lower = group_index * share_width
        part_sum = jnp.dot(mixed[:, lower:lower + share_width], weight[lower:lower + share_width], preferred_element_type=jnp.float32)
        rounded = lax.optimization_barrier(part_sum.astype(jnp.bfloat16))
        total_sum = total_sum + rounded.astype(jnp.float32)
    return total_sum

def reference(residual, query_first, key_first, value_first, documents, bias_first, out_first, norm_gain, query_w, key_w, value_w, bias_second, out_second):
    mixed_one = segment_attention(query_first, key_first, value_first, documents, bias_first)
    layer_one = (residual.astype(jnp.float32) + project_out(mixed_one, out_first)).astype(jnp.bfloat16)
    rows_wide = layer_one.astype(jnp.float32)
    scale = lax.rsqrt(lax.optimization_barrier(jnp.mean(rows_wide * rows_wide, axis=1, keepdims=True)) + eps)
    normed = (rows_wide * scale * norm_gain.astype(jnp.float32)).astype(jnp.bfloat16)
    query_two = jnp.dot(normed, query_w, preferred_element_type=jnp.float32).astype(jnp.bfloat16)
    key_two = jnp.dot(normed, key_w, preferred_element_type=jnp.float32).astype(jnp.bfloat16)
    value_two = jnp.dot(normed, value_w, preferred_element_type=jnp.float32).astype(jnp.bfloat16)
    mixed_two = segment_attention(query_two, key_two, value_two, documents, bias_second)
    return (layer_one.astype(jnp.float32) + project_out(mixed_two, out_second)).astype(jnp.bfloat16)
```

```python
import functools

import jax
import jax.numpy as jnp
from jax import lax
from jax.experimental import pallas as pl
from jax.experimental.pallas import tpu as pltpu
from jax.sharding import PartitionSpec as P

HEAD_SIZE = 64
SEG = 64
PAST = 4
EPS = 1e-06
BAND = SEG * (PAST + 1)
WIDE = 384
TILE = 128
NEG = -1e30
F32 = jnp.float32
BF16 = jnp.bfloat16

GROUP_HEADS = ((0, 2, 5, 7), (1, 3, 4, 6))


def whole():
    return pl.BlockSpec(memory_space=pltpu.VMEM)


def params(mib):
    return pltpu.CompilerParams(vmem_limit_bytes=mib * 1024 * 1024)


def shape(*dims, dtype=BF16):
    return jax.ShapeDtypeStruct(dims, dtype)


def cost(flops, transcendentals=0, nbytes=1 << 20):
    return pl.CostEstimate(flops=flops, bytes_accessed=nbytes, transcendentals=transcendentals)


def from_behind(block, distance):
    devices = range(lax.axis_size("sp"))
    route = [(i - distance, i) for i in devices if i - distance in devices]
    return lax.ppermute(block, "sp", route)


def pack_kernel(key_ref, value_ref, doc_ref, near_ref, far_ref, line):
    rows = key_ref.shape[0]
    near_ref[0:rows, 0:TILE] = key_ref[...]
    near_ref[0:rows, TILE : 2 * TILE] = value_ref[...]
    far_ref[0:SEG, 0:TILE] = key_ref[rows - SEG : rows, :]
    far_ref[0:SEG, TILE : 2 * TILE] = value_ref[rows - SEG : rows, :]
    line[...] = jnp.zeros_like(line)
    codes = (doc_ref[...] + 1).astype(F32)
    line[:, 0:rows] = jnp.broadcast_to(codes, (8, rows))
    flat = line[...]
    lanes = lax.broadcasted_iota(jnp.int32, flat.shape, 1)
    near = pltpu.roll(flat, SEG, 1)
    far = jnp.where(lanes < SEG, pltpu.roll(flat, 2 * TILE - (rows - SEG), 1), 0.0)
    near_ref[rows : rows + 16, :] = jnp.concatenate([near, near], axis=0).astype(BF16)
    far_ref[SEG : SEG + 16, :] = jnp.concatenate([far, far], axis=0).astype(BF16)


def fill_bias(table_ref, bias):
    table = table_ref[:, 0 : 4 * TILE]
    last = table_ref[:, 4 * TILE : 4 * TILE + 1]
    lanes = lax.broadcasted_iota(jnp.int32, table.shape, 1)
    moved = jnp.where(lanes < 448, pltpu.roll(table, 448, 1), jnp.broadcast_to(last, table.shape))
    mirror = 127 - lax.broadcasted_iota(jnp.int32, (8, TILE), 1)
    pieces = [
        jnp.take_along_axis(moved[:, TILE * t : TILE * (t + 1)], mirror, axis=1)
        for t in (3, 2, 1, 0)
    ]
    line = jnp.concatenate(pieces, axis=1)
    for group in range(2):
        for block, head in enumerate(GROUP_HEADS[group]):
            rows = jnp.broadcast_to(line[head : head + 1, :], (SEG, 4 * TILE))
            turned = pltpu.roll(rows, 449, 1, stride=1, stride_axis=0)
            bias[group, SEG * block : SEG * (block + 1), :] = turned[:, 0:WIDE]


def fill_band(src, row, dst, dst_swapped):
    count = src.shape[0]
    dst[row : row + count, :] = src
    for t in range(2):
        part = src[:, TILE * t : TILE * (t + 1)].astype(F32)
        dst_swapped[row : row + count, TILE * t : TILE * (t + 1)] = pltpu.roll(part, SEG, 1).astype(BF16)


def key_codes(doc_ref, near_code, far_code, line):
    rows = doc_ref.shape[1]
    line[...] = jnp.zeros_like(line)
    line[:, 0 : 2 * TILE] = near_code if far_code is None else near_code + far_code
    line[:, 2 * TILE : 2 * TILE + rows] = jnp.broadcast_to((doc_ref[...] + 1).astype(F32), (8, rows))
    return line[...]


def segment_mask(codes, segment):
    turned = codes if segment == 0 else pltpu.roll(codes, 512 - SEG * segment, 1)
    band = jnp.broadcast_to(turned[0:1, 0:WIDE], (SEG, WIDE))
    lanes = lax.broadcasted_iota(jnp.int32, (SEG, WIDE), 1)
    rows = lax.broadcasted_iota(jnp.int32, (SEG, WIDE), 0)
    own = jnp.sum(jnp.where(lanes == rows + PAST * SEG, band, 0.0), axis=1, keepdims=True)
    return jnp.where((band == own) & (lanes < BAND), 0.0, NEG)


def segment_attention(query, band, band_swapped, first_row, mask, bias):
    lanes = lax.broadcasted_iota(jnp.int32, (1, TILE), 1)
    scale = HEAD_SIZE ** (-0.5)
    low = jnp.where(lanes < HEAD_SIZE, scale, 0.0).astype(BF16)
    high = jnp.where(lanes < HEAD_SIZE, 0.0, scale).astype(BF16)
    results = []
    for group in range(2):
        source = band if group == 0 else band_swapped
        keys = source[first_row : first_row + WIDE, 0:TILE]
        values = source[first_row : first_row + WIDE, TILE : 2 * TILE]
        stacked = []
        for tile in range(4):
            even = (tile < 2) == (group == 0)
            stacked.append(query[:, TILE * tile : TILE * (tile + 1)] * (low if even else high))
        left = jnp.concatenate(stacked, axis=0)
        scores = lax.dot_general(left, keys, (((1,), (1,)), ((), ())), preferred_element_type=F32)
        weights = []
        shares = []
        for block in range(4):
            rows = slice(SEG * block, SEG * (block + 1))
            s = scores[rows] + bias[group, rows, :] + mask
            largest = jnp.max(s, axis=1, keepdims=True)
            e = jnp.exp(s - largest)
            shares.append(1.0 / jnp.sum(e, axis=1, keepdims=True))
            weights.append(e.astype(BF16))
        blended = jnp.dot(jnp.concatenate(weights, axis=0), values, preferred_element_type=F32)
        results.append([blended[SEG * b : SEG * (b + 1)] * shares[b] for b in range(4)])
    outs = []
    for tile in range(4):
        even, odd = (0, 1) if tile < 2 else (1, 0)
        outs.append(jnp.where(lanes < HEAD_SIZE, results[even][tile], results[odd][tile]))
    return jnp.concatenate(outs, axis=1)


def later_segments(query, own, near, codes, bias, band, band_swapped, mixed_ref):
    fill_band(near, SEG, band, band_swapped)
    fill_band(own, 4 * SEG, band, band_swapped)
    band[7 * SEG :, :] = jnp.zeros((SEG, 2 * TILE), BF16)
    band_swapped[7 * SEG :, :] = jnp.zeros((SEG, 2 * TILE), BF16)
    for segment in (1, 2):
        out = segment_attention(
            query[SEG * segment : SEG * (segment + 1), :],
            band,
            band_swapped,
            SEG * segment,
            segment_mask(codes, segment),
            bias,
        )
        mixed_ref[SEG * (segment - 1) : SEG * segment, :] = out.astype(BF16)


def first_segment(query, own, near, far, codes, bias, band, band_swapped):
    fill_band(far, 0, band, band_swapped)
    fill_band(near, SEG, band, band_swapped)
    fill_band(own, 4 * SEG, band, band_swapped)
    return segment_attention(query, band, band_swapped, 0, segment_mask(codes, 0), bias).astype(BF16)


def later_one_kernel(query_ref, key_ref, value_ref, doc_ref, near_ref, table_ref, mixed_ref, bias, band, swapped, line):
    rows = key_ref.shape[0]
    fill_bias(table_ref, bias)
    codes = key_codes(doc_ref, near_ref[rows : rows + 8, :].astype(F32), None, line)
    own = jnp.concatenate([key_ref[...], value_ref[...]], axis=1)
    later_segments(query_ref[...], own, near_ref[0:rows, :], codes, bias, band, swapped, mixed_ref)


def first_one_kernel(
    query_ref, key_ref, value_ref, doc_ref, near_ref, far_ref, table_ref, mixed_ref, weight_ref, residual_ref,
    out_ref, bias, band, swapped, line,
):
    rows = key_ref.shape[0]
    fill_bias(table_ref, bias)
    codes = key_codes(
        doc_ref, near_ref[rows : rows + 8, :].astype(F32), far_ref[SEG : SEG + 8, :].astype(F32), line
    )
    own = jnp.concatenate([key_ref[0:TILE, :], value_ref[0:TILE, :]], axis=1)
    head = first_segment(
        query_ref[0:SEG, :], own, near_ref[0:rows, :], far_ref[0:SEG, :], codes, bias, band, swapped
    )
    mixed = jnp.concatenate([head, mixed_ref[...]], axis=0)
    partial = jnp.dot(mixed, weight_ref[...], preferred_element_type=F32)
    mine = (lax.axis_index("tp") == 0).astype(F32)
    residual = residual_ref[...].astype(F32)
    half = residual.shape[1]
    out_ref[:, 0:half] = (partial[:, 0:half] + residual * mine).astype(BF16)
    out_ref[:, half:] = (partial[:, half:] + residual * (1.0 - mine)).astype(BF16)


def norm_kernel(both_ref, gain_ref, key_w_ref, value_w_ref, kv_ref, tail_ref, normed_ref, share_ref):
    layer = (both_ref[0].astype(F32) + both_ref[1].astype(F32)).astype(BF16)
    wide = layer.astype(F32)
    rows, channels = wide.shape
    scale = lax.rsqrt(jnp.mean(wide * wide, axis=1, keepdims=True) + EPS)
    normed = (wide * scale * gain_ref[...]).astype(BF16)
    keys = jnp.dot(normed, key_w_ref[...], preferred_element_type=F32).astype(BF16)
    values = jnp.dot(normed, value_w_ref[...], preferred_element_type=F32).astype(BF16)
    kv_ref[:, 0:TILE] = keys
    kv_ref[:, TILE : 2 * TILE] = values
    tail_ref[:, 0:TILE] = keys[rows - SEG :]
    tail_ref[:, TILE : 2 * TILE] = values[rows - SEG :]
    normed_ref[...] = normed
    half = channels // 2
    share_ref[...] = jnp.where(lax.axis_index("tp") == 0, wide[:, 0:half], wide[:, half:]).astype(BF16)


def later_two_kernel(
    normed_ref, weight_ref, kv_ref, doc_ref, near_ref, codes_ref, table_ref, mixed_ref, head_ref,
    bias, band, swapped, line,
):
    rows = kv_ref.shape[0]
    fill_bias(table_ref, bias)
    query = jnp.dot(normed_ref[...], weight_ref[...], preferred_element_type=F32).astype(BF16)
    head_ref[...] = query[0:SEG, :]
    codes = key_codes(doc_ref, codes_ref[rows : rows + 8, :].astype(F32), None, line)
    later_segments(query, kv_ref[...], near_ref[...], codes, bias, band, swapped, mixed_ref)


def first_two_kernel(
    head_ref, kv_ref, doc_ref, near_ref, far_ref, near_codes_ref, far_codes_ref, table_ref, mixed_ref, weight_ref,
    out_ref, bias, band, swapped, line,
):
    rows = kv_ref.shape[0]
    fill_bias(table_ref, bias)
    codes = key_codes(
        doc_ref, near_codes_ref[rows : rows + 8, :].astype(F32), far_codes_ref[SEG : SEG + 8, :].astype(F32), line
    )
    head = first_segment(
        head_ref[...], kv_ref[0:TILE, :], near_ref[...], far_ref[...], codes, bias, band, swapped
    )
    mixed = jnp.concatenate([head, mixed_ref[...]], axis=0)
    out_ref[...] = jnp.dot(mixed, weight_ref[...], preferred_element_type=F32).astype(BF16)


def last_kernel(both_ref, share_ref, out_ref):
    half = share_ref.shape[1]
    mine = pl.ds(pl.multiple_of(lax.axis_index("tp") * half, half), half)
    out_ref[...] = (
        share_ref[...].astype(F32) + both_ref[0, :, mine].astype(F32) + both_ref[1, :, mine].astype(F32)
    ).astype(BF16)


def call(kernel, outs, scratch, args, flops, mib=16):
    return pl.pallas_call(
        kernel,
        out_shape=outs,
        in_specs=[whole()] * len(args),
        out_specs=jax.tree.map(lambda _: whole(), outs),
        scratch_shapes=scratch,
        compiler_params=params(mib),
        cost_estimate=cost(flops),
    )(*args)


def body(
    residual,
    query_first,
    key_first,
    value_first,
    documents,
    bias_first,
    out_first,
    norm_gain,
    query_w,
    key_w,
    value_w,
    bias_second,
    out_second,
):
    rows, half = residual.shape
    width = query_first.shape[1]
    channels = out_first.shape[1]
    docs = documents.reshape(1, rows)
    gain = norm_gain.reshape(1, channels)
    attention_scratch = [
        pltpu.VMEM((2, 4 * SEG, WIDE), F32),
        pltpu.VMEM((8 * SEG, 2 * TILE), BF16),
        pltpu.VMEM((8 * SEG, 2 * TILE), BF16),
        pltpu.VMEM((8, 4 * TILE), F32),
    ]
    near_send, far_send = call(
        pack_kernel,
        (shape(rows + 16, 2 * TILE), shape(SEG + 16, 2 * TILE)),
        [pltpu.VMEM((8, 2 * TILE), F32)],
        (key_first, value_first, docs),
        1 << 20,
    )
    near_one = from_behind(near_send, 1)
    far_one = from_behind(far_send, 2)
    later_one = call(
        later_one_kernel,
        shape(rows - SEG, width),
        attention_scratch,
        (query_first, key_first, value_first, docs, near_one, bias_first),
        1 << 31,
    )
    sent_one = call(
        first_one_kernel,
        shape(rows, channels),
        attention_scratch,
        (query_first, key_first, value_first, docs, near_one, far_one, bias_first, later_one, out_first, residual),
        1 << 30,
    )
    both_one = lax.all_gather(sent_one, "tp", axis=0)
    kv_two, tail_two, normed, share = call(
        norm_kernel,
        (shape(rows, 2 * TILE), shape(SEG, 2 * TILE), shape(rows, channels), shape(rows, half)),
        [],
        (both_one, gain, key_w, value_w),
        1 << 30,
    )
    near_two = from_behind(kv_two, 1)
    far_two = from_behind(tail_two, 2)
    later_two, head_two = call(
        later_two_kernel,
        (shape(rows - SEG, width), shape(SEG, width)),
        attention_scratch,
        (normed, query_w, kv_two, docs, near_two, near_one, bias_second),
        1 << 31,
    )
    sent_two = call(
        first_two_kernel,
        shape(rows, channels),
        attention_scratch,
        (head_two, kv_two, docs, near_two, far_two, near_one, far_one, bias_second, later_two, out_second),
        1 << 30,
    )
    both_two = lax.all_gather(sent_two, "tp", axis=0)
    return call(last_kernel, shape(rows, half), [], (both_two, share), 1 << 20)


def solution(mesh):
    placed = (
        P("sp", "tp"),
        P("sp", "tp"),
        P("sp", "tp"),
        P("sp", "tp"),
        P("sp"),
        P("tp", None),
        P("tp", None),
        P(),
        P(None, "tp"),
        P(None, "tp"),
        P(None, "tp"),
        P("tp", None),
        P("tp", None),
    )
    return jax.shard_map(body, mesh=mesh, in_specs=placed, out_specs=P("sp", "tp"), check_vma=False)
```

```python
import jax
import jax.numpy as jnp
from jax import lax
from jax.experimental import pallas as pl
from jax.experimental.pallas import tpu as pltpu
from jax.sharding import PartitionSpec as P


HEAD_SIZE = 64
SEG = 64
EPS = 1e-06
TILE = 128
NEG = -1e30
F32 = jnp.float32
BF16 = jnp.bfloat16

GROUP_HEADS = ((0, 2, 5, 7), (1, 3, 4, 6))


def whole():
    return pl.BlockSpec(memory_space=pltpu.VMEM)


def params(mib):
    return pltpu.CompilerParams(vmem_limit_bytes=mib * 1024 * 1024)


def shape(*dims, dtype=BF16):
    return jax.ShapeDtypeStruct(dims, dtype)


def cost(flops, transcendentals=0, nbytes=1 << 20):
    return pl.CostEstimate(flops=flops, bytes_accessed=nbytes, transcendentals=transcendentals)


def from_behind(block, distance):
    devices = range(lax.axis_size("sp"))
    route = [(i - distance, i) for i in devices if i - distance in devices]
    return lax.ppermute(block, "sp", route)


def pack_kernel(key_hbm, value_hbm, doc_hbm, query_hbm, near_ref, far_ref, query_ref, line, docs, sems):
    rows = key_hbm.shape[0]
    copies = [
        (doc_hbm, docs),
        (key_hbm, near_ref.at[0:rows, 0:TILE]),
        (value_hbm, near_ref.at[0:rows, TILE : 2 * TILE]),
        (key_hbm.at[rows - SEG : rows, :], far_ref.at[0:SEG, 0:TILE]),
        (value_hbm.at[rows - SEG : rows, :], far_ref.at[0:SEG, TILE : 2 * TILE]),
        (query_hbm, query_ref),
    ]
    copies = [pltpu.make_async_copy(a, b, sems.at[i]) for i, (a, b) in enumerate(copies)]
    for copy in copies:
        copy.start()
    line[...] = jnp.zeros_like(line)
    copies[0].wait()
    codes = (docs[...] + 1).astype(F32)
    line[:, 0:rows] = jnp.broadcast_to(codes, (8, rows))
    flat = line[...]
    lanes = lax.broadcasted_iota(jnp.int32, flat.shape, 1)
    near = pltpu.roll(flat, SEG, 1)
    far = jnp.where(lanes < SEG, pltpu.roll(flat, 2 * TILE - (rows - SEG), 1), 0.0)
    near_ref[rows : rows + 16, :] = jnp.concatenate([near, near], axis=0).astype(BF16)
    far_ref[SEG : SEG + 16, :] = jnp.concatenate([far, far], axis=0).astype(BF16)
    for copy in copies[1:]:
        copy.wait()


def fill_bias(table_ref, halo_bias, own_bias):
    table = table_ref[:, 0 : 4 * TILE]
    last = table_ref[:, 4 * TILE : 4 * TILE + 1]
    lanes = lax.broadcasted_iota(jnp.int32, table.shape, 1)
    moved = jnp.where(lanes < 448, pltpu.roll(table, 448, 1), jnp.broadcast_to(last, table.shape))
    mirror = 127 - lax.broadcasted_iota(jnp.int32, (8, TILE), 1)
    pieces = [
        jnp.take_along_axis(moved[:, TILE * t : TILE * (t + 1)], mirror, axis=1)
        for t in (3, 2, 1, 0)
    ]
    line = jnp.concatenate(pieces, axis=1)
    for group in range(2):
        for block, head in enumerate(GROUP_HEADS[group]):
            rows = jnp.broadcast_to(line[head : head + 1, :], (SEG, 4 * TILE))
            spot = slice(SEG * block, SEG * (block + 1))
            for odd in range(2):
                turned = pltpu.roll(rows, 449 if odd == 0 else 1, 1, stride=1, stride_axis=0)
                halo_bias[odd, group, spot, :] = turned[:, 0 : 2 * TILE]
                if odd == 0:
                    own_bias[group, spot, 0 : 2 * TILE] = turned[:, TILE : 3 * TILE]
                else:
                    own_bias[group, spot, 2 * TILE : 3 * TILE] = turned[:, 2 * TILE : 3 * TILE]


def swap_halves(part):
    tiles = [
        pltpu.roll(part[:, TILE * t : TILE * (t + 1)].astype(F32), SEG, 1).astype(BF16) for t in range(2)
    ]
    return jnp.concatenate(tiles, axis=1)


def query_code(own_codes, segment):
    lanes = lax.broadcasted_iota(jnp.int32, (SEG, 2 * TILE), 1)
    rows = lax.broadcasted_iota(jnp.int32, (SEG, 2 * TILE), 0)
    spread = jnp.broadcast_to(own_codes[0:1, :], (SEG, 2 * TILE))
    return jnp.sum(jnp.where(lanes == rows + SEG * segment, spread, 0.0), axis=1, keepdims=True)


def code_mask(codes, mine, low, high):
    lanes = lax.broadcasted_iota(jnp.int32, (SEG, codes.shape[1]), 1)
    agree = (jnp.broadcast_to(codes, (SEG, codes.shape[1])) == mine) & (lanes >= low) & (lanes < high)
    return jnp.where(agree, 0.0, NEG)


def half_scales():
    lanes = lax.broadcasted_iota(jnp.int32, (1, TILE), 1)
    scale = HEAD_SIZE ** (-0.5)
    low = jnp.where(lanes < HEAD_SIZE, scale, 0.0).astype(BF16)
    high = jnp.where(lanes < HEAD_SIZE, 0.0, scale).astype(BF16)
    return low, high


def stacked_queries(query, group):
    low, high = half_scales()
    return jnp.concatenate(
        [
            query[:, TILE * t : TILE * (t + 1)] * (low if (t < 2) == (group == 0) else high)
            for t in range(4)
        ],
        axis=0,
    )


def own_part(query, own, codes, own_bias, band, swapped, partial_ref, top_ref, total_ref):
    rows = own.shape[0]
    band[0:rows, :] = own
    band[rows:, :] = jnp.zeros((2 * TILE - rows, 2 * TILE), BF16)
    swapped[0:rows, :] = swap_halves(own)
    swapped[rows:, :] = jnp.zeros((2 * TILE - rows, 2 * TILE), BF16)
    for segment in range(3):
        width = 2 * TILE if segment == 2 else TILE
        first = (TILE, 2 * TILE, 0)[segment]
        mask = code_mask(codes[0:1, 0:width], query_code(codes, segment), 0, SEG * (segment + 1))
        for group in range(2):
            source = band if group == 0 else swapped
            left = stacked_queries(query[SEG * segment : SEG * (segment + 1), :], group)
            scores = lax.dot_general(
                left, source[0:width, 0:TILE], (((1,), (1,)), ((), ())), preferred_element_type=F32
            )
            base = 4 * SEG * (2 * segment + group)
            weights = []
            for block in range(4):
                spot = slice(SEG * block, SEG * (block + 1))
                s = scores[spot] + own_bias[group, spot, first : first + width] + mask
                top = jnp.max(s, axis=1, keepdims=True)
                e = jnp.exp(s - top)
                place = slice(base + SEG * block, base + SEG * (block + 1))
                top_ref[place, :] = jnp.broadcast_to(top, (SEG, TILE))
                total_ref[place, :] = jnp.broadcast_to(jnp.sum(e, axis=1, keepdims=True), (SEG, TILE))
                weights.append(e.astype(BF16))
            partial_ref[base : base + 4 * SEG, :] = jnp.dot(
                jnp.concatenate(weights, axis=0), source[0:width, TILE : 2 * TILE], preferred_element_type=F32
            )


def near_part(query_ref, near, codes, own_codes, halo_bias, partial_ref, top_ref, total_ref, band, swapped, mixed, heads_out):
    for target, rows in ((band, near), (swapped, swap_halves(near))):
        target[0:SEG, :] = jnp.zeros((SEG, 2 * TILE), BF16)
        target[SEG:, :] = rows
    lanes = lax.broadcasted_iota(jnp.int32, (1, TILE), 1)
    head_partial, head_top, head_total = heads_out
    for segment in range(3):
        start = TILE if segment == 2 else 0
        width = 2 * TILE - start
        mask = code_mask(codes[0:1, start:], query_code(own_codes, segment), 0 if segment == 2 else SEG, width)
        results = []
        for group in range(2):
            source = band if group == 0 else swapped
            left = stacked_queries(query_ref[SEG * segment : SEG * (segment + 1), :], group)
            scores = lax.dot_general(
                left, source[start:, 0:TILE], (((1,), (1,)), ((), ())), preferred_element_type=F32
            )
            base = 4 * SEG * (2 * segment + group)
            weights = []
            olds = []
            shares = []
            for block in range(4):
                spot = slice(SEG * block, SEG * (block + 1))
                place = slice(base + SEG * block, base + SEG * (block + 1))
                s = scores[spot] + halo_bias[segment % 2, group, spot, 0:width] + mask
                old_top = top_ref[place, :]
                top = jnp.maximum(jnp.max(s, axis=1, keepdims=True), old_top)
                e = jnp.exp(s - jnp.concatenate([top] * (width // TILE), axis=1))
                old = jnp.exp(old_top - top)
                total = total_ref[place, :] * old + jnp.sum(e, axis=1, keepdims=True)
                weights.append(e.astype(BF16))
                if segment == 0:
                    head_top[place, :] = top
                    head_total[place, :] = total
                    olds.append(old)
                else:
                    share = 1.0 / total
                    shares.append(share)
                    olds.append(old * share)
            blended = jnp.dot(
                jnp.concatenate(weights, axis=0), source[start:, TILE : 2 * TILE], preferred_element_type=F32
            )
            for block in range(4):
                place = slice(base + SEG * block, base + SEG * (block + 1))
                fresh = blended[SEG * block : SEG * (block + 1)]
                before = partial_ref[place, :] * olds[block]
                if segment == 0:
                    head_partial[place, :] = fresh + before
                else:
                    results.append(fresh * shares[block] + before)
        if segment:
            store_heads(mixed, SEG * (segment - 1), results, lanes)


def store_heads(mixed, row, results, lanes):
    for tile in range(4):
        even, odd = (0, 4) if tile < 2 else (4, 0)
        mixed[row : row + SEG, TILE * tile : TILE * (tile + 1)] = jnp.where(
            lanes < HEAD_SIZE, results[even + tile], results[odd + tile]
        ).astype(BF16)


def far_part(query, far, codes, own_codes, halo_bias, partial_ref, top_ref, total_ref, mixed):
    lanes = lax.broadcasted_iota(jnp.int32, (1, TILE), 1)
    mask = code_mask(codes[0:1, 0:SEG], query_code(own_codes, 0), 0, SEG)
    sides = (far, swap_halves(far))
    results = []
    for group in range(2):
        left = stacked_queries(query, group)
        scores = lax.dot_general(
            left, sides[group][:, 0:TILE], (((1,), (1,)), ((), ())), preferred_element_type=F32
        )
        base = 4 * SEG * group
        weights = []
        olds = []
        shares = []
        for block in range(4):
            spot = slice(SEG * block, SEG * (block + 1))
            place = slice(base + SEG * block, base + SEG * (block + 1))
            s = scores[spot] + halo_bias[0, group, spot, 0:SEG] + mask
            old_top = top_ref[place, :]
            top = jnp.maximum(jnp.max(s, axis=1, keepdims=True), old_top)
            e = jnp.exp(s - top[:, 0:SEG])
            old = jnp.exp(old_top - top)
            share = 1.0 / (total_ref[place, :] * old + jnp.sum(e, axis=1, keepdims=True))
            shares.append(share)
            olds.append(old * share)
            weights.append(e.astype(BF16))
        blended = jnp.dot(
            jnp.concatenate(weights, axis=0), sides[group][:, TILE : 2 * TILE], preferred_element_type=F32
        )
        for block in range(4):
            place = slice(base + SEG * block, base + SEG * (block + 1))
            results.append(
                blended[SEG * block : SEG * (block + 1)] * shares[block] + partial_ref[place, :] * olds[block]
            )
    store_heads(mixed, 0, results, lanes)


def codes_of(packed_ref, row, turn):
    codes = packed_ref[row : row + 16, :].astype(F32)[0:8]
    return pltpu.roll(codes, turn, 1) if turn else codes


def before_one_kernel(query_ref, packed_ref, table_ref, halo_bias, partial_ref, top_ref, total_ref, own_bias, band, swapped):
    rows = query_ref.shape[0]
    fill_bias(table_ref, halo_bias, own_bias)
    own_codes = codes_of(packed_ref, rows, 2 * TILE - SEG)
    own_part(
        query_ref[...], packed_ref[0:rows, :], own_codes, own_bias, band, swapped, partial_ref, top_ref, total_ref
    )


def before_two_kernel(
    normed_ref, weight_ref, kv_ref, packed_ref, table_ref, query_ref, halo_bias, partial_ref, top_ref, total_ref,
    own_bias, band, swapped,
):
    rows = kv_ref.shape[0]
    query = jnp.dot(normed_ref[...], weight_ref[...], preferred_element_type=F32).astype(BF16)
    query_ref[...] = query
    fill_bias(table_ref, halo_bias, own_bias)
    own_codes = codes_of(packed_ref, rows, 2 * TILE - SEG)
    own_part(query, kv_ref[...], own_codes, own_bias, band, swapped, partial_ref, top_ref, total_ref)


def with_residual(partial, residual):
    mine = (lax.axis_index("tp") == 0).astype(F32)
    wide = residual.astype(F32)
    half = wide.shape[1]
    return (partial[:, 0:half] + wide * mine).astype(BF16), (partial[:, half:] + wide * (1.0 - mine)).astype(BF16)


def near_one_kernel(
    query_ref, near_ref, packed_ref, halo_bias, partial_ref, top_ref, total_ref, weight_ref, residual_ref,
    out_ref, head_partial, head_top, head_total, band, swapped, mixed,
):
    rows = query_ref.shape[0]
    near_part(
        query_ref, near_ref[0:rows, :], codes_of(near_ref, rows, 0), codes_of(packed_ref, rows, 2 * TILE - SEG),
        halo_bias, partial_ref, top_ref, total_ref, band, swapped, mixed, (head_partial, head_top, head_total),
    )
    partial = jnp.dot(mixed[...], weight_ref[...], preferred_element_type=F32)
    half = residual_ref.shape[1]
    out_ref[:, 0:half], out_ref[:, half:] = with_residual(partial, residual_ref[SEG:, :])


def near_two_kernel(
    query_ref, near_ref, near_codes_ref, packed_ref, halo_bias, partial_ref, top_ref, total_ref, weight_ref,
    out_ref, head_partial, head_top, head_total, band, swapped, mixed,
):
    rows = query_ref.shape[0]
    near_part(
        query_ref, near_ref[...], codes_of(near_codes_ref, rows, 0), codes_of(packed_ref, rows, 2 * TILE - SEG),
        halo_bias, partial_ref, top_ref, total_ref, band, swapped, mixed, (head_partial, head_top, head_total),
    )
    out_ref[...] = jnp.dot(mixed[...], weight_ref[...], preferred_element_type=F32).astype(BF16)


def far_one_kernel(
    query_ref, far_ref, packed_ref, halo_bias, rest_ref, partial_ref, top_ref, total_ref, weight_ref, residual_ref,
    out_ref, mixed,
):
    rows = query_ref.shape[0]
    out_ref[SEG:, :] = rest_ref[...]
    far_part(
        query_ref[0:SEG, :], far_ref[0:SEG, :], codes_of(far_ref, SEG, 0), codes_of(packed_ref, rows, 2 * TILE - SEG),
        halo_bias, partial_ref, top_ref, total_ref, mixed,
    )
    partial = jnp.dot(mixed[...], weight_ref[...], preferred_element_type=F32)
    half = residual_ref.shape[1]
    out_ref[0:SEG, 0:half], out_ref[0:SEG, half:] = with_residual(partial, residual_ref[0:SEG, :])


def far_two_kernel(
    query_ref, far_ref, far_codes_ref, packed_ref, halo_bias, rest_ref, partial_ref, top_ref, total_ref, weight_ref,
    out_ref, mixed,
):
    rows = query_ref.shape[0]
    out_ref[SEG:, :] = rest_ref[...]
    far_part(
        query_ref[0:SEG, :], far_ref[...], codes_of(far_codes_ref, SEG, 0), codes_of(packed_ref, rows, 2 * TILE - SEG),
        halo_bias, partial_ref, top_ref, total_ref, mixed,
    )
    out_ref[0:SEG, :] = jnp.dot(mixed[...], weight_ref[...], preferred_element_type=F32).astype(BF16)


def norm_kernel(both_ref, gain_ref, key_w_ref, value_w_ref, kv_ref, tail_ref, normed_ref, share_ref):
    layer = (both_ref[0].astype(F32) + both_ref[1].astype(F32)).astype(BF16)
    wide = layer.astype(F32)
    rows, channels = wide.shape
    scale = lax.rsqrt(jnp.mean(wide * wide, axis=1, keepdims=True) + EPS)
    normed = (wide * scale * gain_ref[...]).astype(BF16)
    keys = jnp.dot(normed, key_w_ref[...], preferred_element_type=F32).astype(BF16)
    values = jnp.dot(normed, value_w_ref[...], preferred_element_type=F32).astype(BF16)
    kv_ref[:, 0:TILE] = keys
    kv_ref[:, TILE : 2 * TILE] = values
    tail_ref[:, 0:TILE] = keys[rows - SEG :]
    tail_ref[:, TILE : 2 * TILE] = values[rows - SEG :]
    normed_ref[...] = normed
    half = channels // 2
    share_ref[...] = jnp.where(lax.axis_index("tp") == 0, wide[:, 0:half], wide[:, half:]).astype(BF16)


def last_kernel(both_ref, share_ref, out_ref):
    half = share_ref.shape[1]
    mine = pl.ds(pl.multiple_of(lax.axis_index("tp") * half, half), half)
    out_ref[...] = (
        share_ref[...].astype(F32) + both_ref[0, :, mine].astype(F32) + both_ref[1, :, mine].astype(F32)
    ).astype(BF16)


def call(kernel, outs, scratch, args, flops, mib=16, spaces=None):
    return pl.pallas_call(
        kernel,
        out_shape=outs,
        in_specs=[whole()] * len(args) if spaces is None else [pl.BlockSpec(memory_space=s) for s in spaces],
        out_specs=jax.tree.map(lambda _: whole(), outs),
        scratch_shapes=scratch,
        compiler_params=params(mib),
        cost_estimate=cost(flops),
    )(*args)


def body(
    residual,
    query_first,
    key_first,
    value_first,
    documents,
    bias_first,
    out_first,
    norm_gain,
    query_w,
    key_w,
    value_w,
    bias_second,
    out_second,
):
    rows, half = residual.shape
    width = query_first.shape[1]
    channels = out_first.shape[1]
    docs = documents.reshape(1, rows)
    gain = norm_gain.reshape(1, channels)
    bands = [pltpu.VMEM((2 * TILE, 2 * TILE), BF16), pltpu.VMEM((2 * TILE, 2 * TILE), BF16)]
    before_scratch = [pltpu.VMEM((2, 4 * SEG, 3 * TILE), F32), *bands]
    near_scratch = [*bands, pltpu.VMEM((rows - SEG, width), BF16)]
    far_scratch = [pltpu.VMEM((SEG, width), BF16)]
    stats = shape(24 * SEG, TILE, dtype=F32)
    head_stats = shape(8 * SEG, TILE, dtype=F32)
    near_shapes = (shape(rows - SEG, channels), head_stats, head_stats, head_stats)
    own_shapes = (shape(2, 2, 4 * SEG, 2 * TILE, dtype=F32), stats, stats, stats)
    packed, far_send, query_one = call(
        pack_kernel,
        (shape(rows + 16, 2 * TILE), shape(SEG + 16, 2 * TILE), shape(rows, width)),
        [pltpu.VMEM((8, 2 * TILE), F32), pltpu.VMEM((1, rows), jnp.int32), pltpu.SemaphoreType.DMA((6,))],
        tuple(pltpu.with_memory_space_constraint(x, pltpu.HBM) for x in (key_first, value_first, docs, query_first)),
        1 << 20,
        spaces=[pltpu.HBM] * 4,
    )
    near_one = from_behind(packed, 1)
    far_one = from_behind(far_send, 2)
    own_one = call(
        before_one_kernel, own_shapes, before_scratch, (query_one, packed, bias_first), 1 << 31
    )
    rest_one = call(
        near_one_kernel,
        near_shapes,
        near_scratch,
        (query_one, near_one, packed, *own_one, out_first, residual),
        1 << 31,
    )
    sent_one = call(
        far_one_kernel,
        shape(rows, channels),
        far_scratch,
        (query_one, far_one, packed, own_one[0], *rest_one, out_first, residual),
        1 << 31,
    )
    both_one = lax.all_gather(sent_one, "tp", axis=0)
    kv_two, tail_two, normed, share = call(
        norm_kernel,
        (shape(rows, 2 * TILE), shape(SEG, 2 * TILE), shape(rows, channels), shape(rows, half)),
        [],
        (both_one, gain, key_w, value_w),
        1 << 30,
    )
    near_two = from_behind(kv_two, 1)
    far_two = from_behind(tail_two, 2)
    query_two, *own_two = call(
        before_two_kernel,
        (shape(rows, width), *own_shapes),
        before_scratch,
        (normed, query_w, kv_two, packed, bias_second),
        1 << 31,
    )
    rest_two = call(
        near_two_kernel,
        near_shapes,
        near_scratch,
        (query_two, near_two, near_one, packed, *own_two, out_second),
        1 << 31,
    )
    sent_two = call(
        far_two_kernel,
        shape(rows, channels),
        far_scratch,
        (query_two, far_two, far_one, packed, own_two[0], *rest_two, out_second),
        1 << 31,
    )
    both_two = lax.all_gather(sent_two, "tp", axis=0)
    return call(last_kernel, shape(rows, half), [], (both_two, share), 1 << 20)


def solution(mesh):
    placed = (
        P("sp", "tp"),
        P("sp", "tp"),
        P("sp", "tp"),
        P("sp", "tp"),
        P("sp"),
        P("tp", None),
        P("tp", None),
        P(),
        P(None, "tp"),
        P(None, "tp"),
        P(None, "tp"),
        P("tp", None),
        P("tp", None),
    )
    return jax.shard_map(body, mesh=mesh, in_specs=placed, out_specs=P("sp", "tp"), check_vma=False)
```

```python
import jax
import jax.numpy as jnp
from jax import lax
from jax.experimental import pallas as pl
from jax.experimental.pallas import tpu as pltpu
from jax.sharding import PartitionSpec as P


HEAD_SIZE = 64
SEG = 64
EPS = 1e-06
TILE = 128
NEG = -1e30
F32 = jnp.float32
BF16 = jnp.bfloat16

GROUP_HEADS = ((0, 2, 5, 7), (1, 3, 4, 6))


def whole():
    return pl.BlockSpec(memory_space=pltpu.VMEM)


def params(mib):
    return pltpu.CompilerParams(vmem_limit_bytes=mib * 1024 * 1024)


def shape(*dims, dtype=BF16):
    return jax.ShapeDtypeStruct(dims, dtype)


def cost(flops, transcendentals=0, nbytes=1 << 20):
    return pl.CostEstimate(flops=flops, bytes_accessed=nbytes, transcendentals=transcendentals)


def from_behind(block, distance):
    devices = range(lax.axis_size("sp"))
    route = [(i - distance, i) for i in devices if i - distance in devices]
    return lax.ppermute(block, "sp", route)


def pack_kernel(key_hbm, value_hbm, doc_hbm, near_ref, far_ref, line, docs, sems):
    rows = key_hbm.shape[0]
    copies = [
        (doc_hbm, docs),
        *(
            (source.at[first : first + rows // 2, :], near_ref.at[first : first + rows // 2, lane : lane + TILE])
            for first in (0, rows // 2)
            for source, lane in ((key_hbm, 0), (value_hbm, TILE))
        ),
        (key_hbm.at[rows - SEG : rows, :], far_ref.at[0:SEG, 0:TILE]),
        (value_hbm.at[rows - SEG : rows, :], far_ref.at[0:SEG, TILE : 2 * TILE]),
    ]
    copies = [pltpu.make_async_copy(a, b, sems.at[i]) for i, (a, b) in enumerate(copies)]
    for copy in copies:
        copy.start()
    line[...] = jnp.zeros_like(line)
    copies[0].wait()
    codes = (docs[...] + 1).astype(F32)
    line[:, 0:rows] = jnp.broadcast_to(codes, (8, rows))
    flat = line[...]
    lanes = lax.broadcasted_iota(jnp.int32, flat.shape, 1)
    near = pltpu.roll(flat, SEG, 1)
    far = jnp.where(lanes < SEG, pltpu.roll(flat, 2 * TILE - (rows - SEG), 1), 0.0)
    near_ref[rows : rows + 16, :] = jnp.concatenate([near, near], axis=0).astype(BF16)
    far_ref[SEG : SEG + 16, :] = jnp.concatenate([far, far], axis=0).astype(BF16)
    for copy in copies[1:]:
        copy.wait()


def fill_bias(table_ref, halo_bias, own_bias):
    table = table_ref[:, 0 : 4 * TILE]
    last = table_ref[:, 4 * TILE : 4 * TILE + 1]
    lanes = lax.broadcasted_iota(jnp.int32, table.shape, 1)
    moved = jnp.where(lanes < 448, pltpu.roll(table, 448, 1), jnp.broadcast_to(last, table.shape))
    mirror = 127 - lax.broadcasted_iota(jnp.int32, (8, TILE), 1)
    pieces = [
        jnp.take_along_axis(moved[:, TILE * t : TILE * (t + 1)], mirror, axis=1)
        for t in (3, 2, 1, 0)
    ]
    line = jnp.concatenate(pieces, axis=1)
    for group in range(2):
        for block, head in enumerate(GROUP_HEADS[group]):
            rows = jnp.broadcast_to(line[head : head + 1, :], (SEG, 4 * TILE))
            spot = slice(SEG * block, SEG * (block + 1))
            for odd in range(2):
                turned = pltpu.roll(rows, 449 if odd == 0 else 1, 1, stride=1, stride_axis=0)
                halo_bias[odd, group, spot, :] = turned[:, 0 : 2 * TILE]
                if odd == 0:
                    own_bias[group, spot, 0 : 2 * TILE] = turned[:, TILE : 3 * TILE]
                else:
                    own_bias[group, spot, 2 * TILE : 3 * TILE] = turned[:, 2 * TILE : 3 * TILE]


def swap_halves(part):
    tiles = [
        pltpu.roll(part[:, TILE * t : TILE * (t + 1)].astype(F32), SEG, 1).astype(BF16) for t in range(2)
    ]
    return jnp.concatenate(tiles, axis=1)


def query_code(own_codes, segment):
    lanes = lax.broadcasted_iota(jnp.int32, (SEG, 2 * TILE), 1)
    rows = lax.broadcasted_iota(jnp.int32, (SEG, 2 * TILE), 0)
    spread = jnp.broadcast_to(own_codes[0:1, :], (SEG, 2 * TILE))
    return jnp.sum(jnp.where(lanes == rows + SEG * segment, spread, 0.0), axis=1, keepdims=True)


def code_mask(codes, mine, low, high):
    lanes = lax.broadcasted_iota(jnp.int32, (SEG, codes.shape[1]), 1)
    agree = (jnp.broadcast_to(codes, (SEG, codes.shape[1])) == mine) & (lanes >= low) & (lanes < high)
    return jnp.where(agree, 0.0, NEG)


def half_scales():
    lanes = lax.broadcasted_iota(jnp.int32, (1, TILE), 1)
    scale = HEAD_SIZE ** (-0.5)
    low = jnp.where(lanes < HEAD_SIZE, scale, 0.0).astype(BF16)
    high = jnp.where(lanes < HEAD_SIZE, 0.0, scale).astype(BF16)
    return low, high


def stacked_queries(query, group):
    low, high = half_scales()
    return jnp.concatenate(
        [
            query[:, TILE * t : TILE * (t + 1)] * (low if (t < 2) == (group == 0) else high)
            for t in range(4)
        ],
        axis=0,
    )


def own_part(query, own, codes, own_bias, band, swapped, partial_ref, top_ref, total_ref):
    rows = own.shape[0]
    band[0:rows, :] = own
    band[rows:, :] = jnp.zeros((2 * TILE - rows, 2 * TILE), BF16)
    swapped[0:rows, :] = swap_halves(own)
    swapped[rows:, :] = jnp.zeros((2 * TILE - rows, 2 * TILE), BF16)
    for segment in range(3):
        width = 2 * TILE if segment == 2 else TILE
        first = (TILE, 2 * TILE, 0)[segment]
        mask = code_mask(codes[0:1, 0:width], query_code(codes, segment), 0, SEG * (segment + 1))
        for group in range(2):
            source = band if group == 0 else swapped
            left = stacked_queries(query[SEG * segment : SEG * (segment + 1), :], group)
            scores = lax.dot_general(
                left, source[0:width, 0:TILE], (((1,), (1,)), ((), ())), preferred_element_type=F32
            )
            base = 4 * SEG * (2 * segment + group)
            weights = []
            for block in range(4):
                spot = slice(SEG * block, SEG * (block + 1))
                s = scores[spot] + own_bias[group, spot, first : first + width] + mask
                top = jnp.max(s, axis=1, keepdims=True)
                e = jnp.exp(s - top)
                place = slice(base + SEG * block, base + SEG * (block + 1))
                top_ref[place, :] = jnp.broadcast_to(top, (SEG, TILE))
                total_ref[place, :] = jnp.broadcast_to(jnp.sum(e, axis=1, keepdims=True), (SEG, TILE))
                weights.append(e.astype(BF16))
            partial_ref[base : base + 4 * SEG, :] = jnp.dot(
                jnp.concatenate(weights, axis=0), source[0:width, TILE : 2 * TILE], preferred_element_type=F32
            )


def near_part(query_ref, near, codes, own_codes, halo_bias, partial_ref, top_ref, total_ref, band, swapped, mixed, heads_out):
    for target, rows in ((band, near), (swapped, swap_halves(near))):
        target[0:SEG, :] = jnp.zeros((SEG, 2 * TILE), BF16)
        target[SEG:, :] = rows
    lanes = lax.broadcasted_iota(jnp.int32, (1, TILE), 1)
    head_partial, head_top, head_total, head_left, head_code = heads_out
    for segment in range(3):
        start = TILE if segment == 2 else 0
        width = 2 * TILE - start
        mine = query_code(own_codes, segment)
        if segment == 0:
            head_code[...] = jnp.broadcast_to(mine, (SEG, TILE))
        mask = code_mask(codes[0:1, start:], mine, 0 if segment == 2 else SEG, width)
        results = []
        for group in range(2):
            source = band if group == 0 else swapped
            left = stacked_queries(query_ref[SEG * segment : SEG * (segment + 1), :], group)
            if segment == 0:
                turned = pltpu.roll(left.astype(F32), SEG, 1).astype(BF16) if group else left
                head_left[4 * SEG * group : 4 * SEG * (group + 1), :] = turned
            scores = lax.dot_general(
                left, source[start:, 0:TILE], (((1,), (1,)), ((), ())), preferred_element_type=F32
            )
            base = 4 * SEG * (2 * segment + group)
            weights = []
            olds = []
            shares = []
            for block in range(4):
                spot = slice(SEG * block, SEG * (block + 1))
                place = slice(base + SEG * block, base + SEG * (block + 1))
                s = scores[spot] + halo_bias[segment % 2, group, spot, 0:width] + mask
                old_top = top_ref[place, :]
                top = jnp.maximum(jnp.max(s, axis=1, keepdims=True), old_top)
                e = jnp.exp(s - jnp.concatenate([top] * (width // TILE), axis=1))
                old = jnp.exp(old_top - top)
                total = total_ref[place, :] * old + jnp.sum(e, axis=1, keepdims=True)
                weights.append(e.astype(BF16))
                if segment == 0:
                    head_top[place, :] = top
                    head_total[place, :] = total
                    olds.append(old)
                else:
                    share = 1.0 / total
                    shares.append(share)
                    olds.append(old * share)
            blended = jnp.dot(
                jnp.concatenate(weights, axis=0), source[start:, TILE : 2 * TILE], preferred_element_type=F32
            )
            for block in range(4):
                place = slice(base + SEG * block, base + SEG * (block + 1))
                fresh = blended[SEG * block : SEG * (block + 1)]
                before = partial_ref[place, :] * olds[block]
                if segment == 0:
                    head_partial[place, :] = fresh + before
                else:
                    results.append(fresh * shares[block] + before)
        if segment:
            store_heads(mixed, SEG * (segment - 1), results, lanes)


def store_heads(mixed, row, results, lanes):
    for tile in range(4):
        even, odd = (0, 4) if tile < 2 else (4, 0)
        mixed[row : row + SEG, TILE * tile : TILE * (tile + 1)] = jnp.where(
            lanes < HEAD_SIZE, results[even + tile], results[odd + tile]
        ).astype(BF16)


def far_part(far, codes, halo_bias, partial_ref, top_ref, total_ref, left_ref, code_ref, mixed):
    lanes = lax.broadcasted_iota(jnp.int32, (1, TILE), 1)
    scores = lax.dot_general(
        left_ref[...], far[:, 0:TILE], (((1,), (1,)), ((), ())), preferred_element_type=F32
    )
    values = far[:, TILE : 2 * TILE]
    both = jnp.concatenate([values, pltpu.roll(values.astype(F32), SEG, 1).astype(BF16)], axis=1)
    agree = jnp.broadcast_to(codes[0:1, 0:SEG], (SEG, SEG)) == code_ref[:, 0:SEG]
    mask = jnp.where(agree, 0.0, NEG)
    weights = []
    olds = []
    shares = []
    for block in range(8):
        spot = slice(SEG * (block % 4), SEG * (block % 4 + 1))
        place = slice(SEG * block, SEG * (block + 1))
        s = scores[place] + halo_bias[0, block // 4, spot, 0:SEG] + mask
        old_top = top_ref[place, :]
        top = jnp.maximum(jnp.max(s, axis=1, keepdims=True), old_top)
        e = jnp.exp(s - top[:, 0:SEG])
        old = jnp.exp(old_top - top)
        share = 1.0 / (total_ref[place, :] * old + jnp.sum(e, axis=1, keepdims=True))
        shares.append(share)
        olds.append(old * share)
        weights.append(e.astype(BF16))
    blended = jnp.dot(jnp.concatenate(weights, axis=0), both, preferred_element_type=F32)
    results = []
    for block in range(8):
        place = slice(SEG * block, SEG * (block + 1))
        side = slice(TILE * (block // 4), TILE * (block // 4 + 1))
        results.append(blended[place, side] * shares[block] + partial_ref[place, :] * olds[block])
    store_heads(mixed, 0, results, lanes)


def codes_of(packed_ref, row, turn):
    codes = packed_ref[row : row + 16, :].astype(F32)[0:8]
    return pltpu.roll(codes, turn, 1) if turn else codes


def before_one_kernel(
    query_hbm, packed_ref, table_ref, query_ref, halo_bias, partial_ref, top_ref, total_ref, own_bias, band, swapped, sem
):
    rows = query_ref.shape[0]
    copy = pltpu.make_async_copy(query_hbm, query_ref, sem)
    copy.start()
    fill_bias(table_ref, halo_bias, own_bias)
    own_codes = codes_of(packed_ref, rows, 2 * TILE - SEG)
    copy.wait()
    own_part(
        query_ref[...], packed_ref[0:rows, :], own_codes, own_bias, band, swapped, partial_ref, top_ref, total_ref
    )


def before_two_kernel(
    normed_ref, weight_ref, kv_ref, packed_ref, table_ref, query_ref, halo_bias, partial_ref, top_ref, total_ref,
    own_bias, band, swapped,
):
    rows = kv_ref.shape[0]
    query = jnp.dot(normed_ref[...], weight_ref[...], preferred_element_type=F32).astype(BF16)
    query_ref[...] = query
    fill_bias(table_ref, halo_bias, own_bias)
    own_codes = codes_of(packed_ref, rows, 2 * TILE - SEG)
    own_part(query, kv_ref[...], own_codes, own_bias, band, swapped, partial_ref, top_ref, total_ref)


def with_residual(partial, residual):
    mine = (lax.axis_index("tp") == 0).astype(F32)
    wide = residual.astype(F32)
    half = wide.shape[1]
    return (partial[:, 0:half] + wide * mine).astype(BF16), (partial[:, half:] + wide * (1.0 - mine)).astype(BF16)


def near_one_kernel(
    query_ref, near_ref, packed_ref, halo_bias, partial_ref, top_ref, total_ref, weight_ref, residual_ref,
    out_ref, head_partial, head_top, head_total, head_left, head_code, band, swapped, mixed,
):
    rows = query_ref.shape[0]
    near_part(
        query_ref, near_ref[0:rows, :], codes_of(near_ref, rows, 0), codes_of(packed_ref, rows, 2 * TILE - SEG),
        halo_bias, partial_ref, top_ref, total_ref, band, swapped, mixed,
        (head_partial, head_top, head_total, head_left, head_code),
    )
    partial = jnp.dot(mixed[...], weight_ref[...], preferred_element_type=F32)
    half = residual_ref.shape[1]
    out_ref[:, 0:half], out_ref[:, half:] = with_residual(partial, residual_ref[SEG:, :])


def near_two_kernel(
    query_ref, near_ref, near_codes_ref, packed_ref, halo_bias, partial_ref, top_ref, total_ref, weight_ref,
    out_ref, head_partial, head_top, head_total, head_left, head_code, band, swapped, mixed,
):
    rows = query_ref.shape[0]
    near_part(
        query_ref, near_ref[...], codes_of(near_codes_ref, rows, 0), codes_of(packed_ref, rows, 2 * TILE - SEG),
        halo_bias, partial_ref, top_ref, total_ref, band, swapped, mixed,
        (head_partial, head_top, head_total, head_left, head_code),
    )
    out_ref[...] = jnp.dot(mixed[...], weight_ref[...], preferred_element_type=F32).astype(BF16)


def far_one_kernel(
    far_ref, halo_bias, rest_ref, partial_ref, top_ref, total_ref, left_ref, code_ref, weight_ref, residual_ref,
    out_ref, mixed,
):
    out_ref[SEG:, :] = rest_ref[...]
    far_part(
        far_ref[0:SEG, :], codes_of(far_ref, SEG, 0), halo_bias, partial_ref, top_ref, total_ref, left_ref, code_ref, mixed
    )
    partial = jnp.dot(mixed[...], weight_ref[...], preferred_element_type=F32)
    half = residual_ref.shape[1]
    out_ref[0:SEG, 0:half], out_ref[0:SEG, half:] = with_residual(partial, residual_ref[0:SEG, :])


def far_two_kernel(
    far_ref, far_codes_ref, halo_bias, rest_ref, partial_ref, top_ref, total_ref, left_ref, code_ref, weight_ref,
    mine_ref, theirs_ref, mixed,
):
    half = mine_ref.shape[1]
    first = lax.axis_index("tp") == 0
    rest = rest_ref[...]
    mine_ref[SEG:, :] = jnp.where(first, rest[:, 0:half], rest[:, half:])
    theirs_ref[SEG:, :] = jnp.where(first, rest[:, half:], rest[:, 0:half])
    far_part(
        far_ref[...], codes_of(far_codes_ref, SEG, 0), halo_bias, partial_ref, top_ref, total_ref, left_ref, code_ref, mixed
    )
    partial = jnp.dot(mixed[...], weight_ref[...], preferred_element_type=F32).astype(BF16)
    mine_ref[0:SEG, :] = jnp.where(first, partial[:, 0:half], partial[:, half:])
    theirs_ref[0:SEG, :] = jnp.where(first, partial[:, half:], partial[:, 0:half])


def norm_kernel(both_ref, gain_ref, key_w_ref, value_w_ref, kv_ref, tail_ref, normed_ref, share_ref):
    layer = (both_ref[0].astype(F32) + both_ref[1].astype(F32)).astype(BF16)
    wide = layer.astype(F32)
    rows, channels = wide.shape
    scale = lax.rsqrt(jnp.mean(wide * wide, axis=1, keepdims=True) + EPS)
    normed = (wide * scale * gain_ref[...]).astype(BF16)
    keys = jnp.dot(normed, key_w_ref[...], preferred_element_type=F32).astype(BF16)
    values = jnp.dot(normed, value_w_ref[...], preferred_element_type=F32).astype(BF16)
    kv_ref[:, 0:TILE] = keys
    kv_ref[:, TILE : 2 * TILE] = values
    tail_ref[:, 0:TILE] = keys[rows - SEG :]
    tail_ref[:, TILE : 2 * TILE] = values[rows - SEG :]
    normed_ref[...] = normed
    half = channels // 2
    share_ref[...] = jnp.where(lax.axis_index("tp") == 0, wide[:, 0:half], wide[:, half:]).astype(BF16)


def last_kernel(both_ref, mine_ref, share_ref, out_hbm, out, sems):
    first = lax.axis_index("tp") == 0
    copies = []
    parts = sems.shape[0]
    rows = out.shape[0] // parts
    for part in range(parts):
        spot = slice(rows * part, rows * (part + 1))
        theirs = jnp.where(first, both_ref[1, spot, :], both_ref[0, spot, :])
        out[spot, :] = (
            share_ref[spot, :].astype(F32) + mine_ref[spot, :].astype(F32) + theirs.astype(F32)
        ).astype(BF16)
        copies.append(pltpu.make_async_copy(out.at[spot, :], out_hbm.at[spot, :], sems.at[part]))
        copies[-1].start()
    for copy in copies:
        copy.wait()


def call(kernel, outs, scratch, args, flops, mib=16, spaces=None, out_space=pltpu.VMEM):
    return pl.pallas_call(
        kernel,
        out_shape=outs,
        in_specs=[whole()] * len(args) if spaces is None else [pl.BlockSpec(memory_space=s) for s in spaces],
        out_specs=jax.tree.map(lambda _: pl.BlockSpec(memory_space=out_space), outs),
        scratch_shapes=scratch,
        compiler_params=params(mib),
        cost_estimate=cost(flops),
    )(*args)


def body(
    residual,
    query_first,
    key_first,
    value_first,
    documents,
    bias_first,
    out_first,
    norm_gain,
    query_w,
    key_w,
    value_w,
    bias_second,
    out_second,
):
    rows, half = residual.shape
    width = query_first.shape[1]
    channels = out_first.shape[1]
    docs = documents.reshape(1, rows)
    gain = norm_gain.reshape(1, channels)
    bands = [pltpu.VMEM((2 * TILE, 2 * TILE), BF16), pltpu.VMEM((2 * TILE, 2 * TILE), BF16)]
    before_scratch = [pltpu.VMEM((2, 4 * SEG, 3 * TILE), F32), *bands]
    near_scratch = [*bands, pltpu.VMEM((rows - SEG, width), BF16)]
    far_scratch = [pltpu.VMEM((SEG, width), BF16)]
    stats = shape(24 * SEG, TILE, dtype=F32)
    head_stats = shape(8 * SEG, TILE, dtype=F32)
    near_shapes = (
        shape(rows - SEG, channels),
        head_stats,
        head_stats,
        head_stats,
        shape(8 * SEG, TILE),
        shape(SEG, TILE, dtype=F32),
    )
    own_shapes = (shape(2, 2, 4 * SEG, 2 * TILE, dtype=F32), stats, stats, stats)
    packed, far_send = call(
        pack_kernel,
        (shape(rows + 16, 2 * TILE), shape(SEG + 16, 2 * TILE)),
        [pltpu.VMEM((8, 2 * TILE), F32), pltpu.VMEM((1, rows), jnp.int32), pltpu.SemaphoreType.DMA((7,))],
        tuple(pltpu.with_memory_space_constraint(x, pltpu.HBM) for x in (key_first, value_first, docs)),
        1 << 20,
        spaces=[pltpu.HBM] * 3,
    )
    near_one = from_behind(packed, 1)
    far_one = from_behind(far_send, 2)
    query_one, *own_one = call(
        before_one_kernel,
        (shape(rows, width), *own_shapes),
        [*before_scratch, pltpu.SemaphoreType.DMA],
        (pltpu.with_memory_space_constraint(query_first, pltpu.HBM), packed, bias_first),
        1 << 31,
        spaces=[pltpu.HBM, pltpu.VMEM, pltpu.VMEM],
    )
    rest_one = call(
        near_one_kernel,
        near_shapes,
        near_scratch,
        (query_one, near_one, packed, *own_one, out_first, residual),
        1 << 31,
    )
    sent_one = call(
        far_one_kernel,
        shape(rows, channels),
        far_scratch,
        (far_one, own_one[0], *rest_one, out_first, residual),
        1 << 31,
    )
    both_one = lax.all_gather(sent_one, "tp", axis=0)
    kv_two, tail_two, normed, share = call(
        norm_kernel,
        (shape(rows, 2 * TILE), shape(SEG, 2 * TILE), shape(rows, channels), shape(rows, half)),
        [],
        (both_one, gain, key_w, value_w),
        1 << 30,
    )
    near_two = from_behind(kv_two, 1)
    far_two = from_behind(tail_two, 2)
    query_two, *own_two = call(
        before_two_kernel,
        (shape(rows, width), *own_shapes),
        before_scratch,
        (normed, query_w, kv_two, packed, bias_second),
        1 << 31,
    )
    rest_two = call(
        near_two_kernel,
        near_shapes,
        near_scratch,
        (query_two, near_two, near_one, packed, *own_two, out_second),
        1 << 31,
    )
    mine_two, sent_two = call(
        far_two_kernel,
        (shape(rows, half), shape(rows, half)),
        far_scratch,
        (far_two, far_one, own_two[0], *rest_two, out_second),
        1 << 31,
    )
    both_two = lax.all_gather(sent_two, "tp", axis=0)
    return call(
        last_kernel,
        shape(rows, half),
        [pltpu.VMEM((rows, half), BF16), pltpu.SemaphoreType.DMA((4,))],
        (both_two, mine_two, share),
        1 << 20,
        out_space=pltpu.HBM,
    )


def solution(mesh):
    placed = (
        P("sp", "tp"),
        P("sp", "tp"),
        P("sp", "tp"),
        P("sp", "tp"),
        P("sp"),
        P("tp", None),
        P("tp", None),
        P(),
        P(None, "tp"),
        P(None, "tp"),
        P(None, "tp"),
        P("tp", None),
        P("tp", None),
    )
    return jax.shard_map(body, mesh=mesh, in_specs=placed, out_specs=P("sp", "tp"), check_vma=False)
```

```python
import jax
import jax.numpy as jnp
from jax import lax
from jax.experimental import pallas as pl
from jax.experimental.pallas import tpu as pltpu
from jax.sharding import PartitionSpec as P


HEAD_SIZE = 64
SEG = 64
EPS = 1e-06
TILE = 128
NEG = -1e30
F32 = jnp.float32
BF16 = jnp.bfloat16

GROUP_HEADS = ((0, 2, 5, 7), (1, 3, 4, 6))


def whole():
    return pl.BlockSpec(memory_space=pltpu.VMEM)


def params(mib):
    return pltpu.CompilerParams(vmem_limit_bytes=mib * 1024 * 1024)


def shape(*dims, dtype=BF16):
    return jax.ShapeDtypeStruct(dims, dtype)


def cost(flops, transcendentals=0, nbytes=1 << 20):
    return pl.CostEstimate(flops=flops, bytes_accessed=nbytes, transcendentals=transcendentals)


def from_behind(block, distance, across=False):
    devices = range(lax.axis_size("sp"))
    route = [(i - distance, i) for i in devices if i - distance in devices]
    if across:
        return lax.ppermute(
            block, ("sp", "tp"), [(2 * a + core, 2 * b + 1 - core) for a, b in route for core in range(2)]
        )
    return lax.ppermute(block, "sp", route)


def pack_kernel(key_hbm, value_hbm, doc_hbm, near_ref, far_ref, line, docs, sems):
    rows = key_hbm.shape[0]
    copies = [
        (doc_hbm, docs),
        *(
            (source.at[first : first + rows // 2, :], near_ref.at[first : first + rows // 2, lane : lane + TILE])
            for first in (0, rows // 2)
            for source, lane in ((key_hbm, 0), (value_hbm, TILE))
        ),
        (key_hbm.at[rows - SEG : rows, :], far_ref.at[0:SEG, 0:TILE]),
        (value_hbm.at[rows - SEG : rows, :], far_ref.at[0:SEG, TILE : 2 * TILE]),
    ]
    copies = [pltpu.make_async_copy(a, b, sems.at[i]) for i, (a, b) in enumerate(copies)]
    for copy in copies:
        copy.start()
    line[...] = jnp.zeros_like(line)
    copies[0].wait()
    codes = (docs[...] + 1).astype(F32)
    line[:, 0:rows] = jnp.broadcast_to(codes, (8, rows))
    flat = line[...]
    lanes = lax.broadcasted_iota(jnp.int32, flat.shape, 1)
    near = pltpu.roll(flat, SEG, 1)
    far = jnp.where(lanes < SEG, pltpu.roll(flat, 2 * TILE - (rows - SEG), 1), 0.0)
    near_ref[rows : rows + 16, :] = jnp.concatenate([near, near], axis=0).astype(BF16)
    far_ref[SEG : SEG + 16, :] = jnp.concatenate([far, far], axis=0).astype(BF16)
    for copy in copies[1:]:
        copy.wait()


def fill_bias(table_ref, halo_bias, own_bias):
    table = table_ref[:, 0 : 4 * TILE]
    last = table_ref[:, 4 * TILE : 4 * TILE + 1]
    lanes = lax.broadcasted_iota(jnp.int32, table.shape, 1)
    moved = jnp.where(lanes < 448, pltpu.roll(table, 448, 1), jnp.broadcast_to(last, table.shape))
    mirror = 127 - lax.broadcasted_iota(jnp.int32, (8, TILE), 1)
    pieces = [
        jnp.take_along_axis(moved[:, TILE * t : TILE * (t + 1)], mirror, axis=1)
        for t in (3, 2, 1, 0)
    ]
    line = jnp.concatenate(pieces, axis=1)
    for group in range(2):
        for block, head in enumerate(GROUP_HEADS[group]):
            rows = jnp.broadcast_to(line[head : head + 1, :], (SEG, 4 * TILE))
            spot = slice(SEG * block, SEG * (block + 1))
            for odd in range(2):
                turned = pltpu.roll(rows, 449 if odd == 0 else 1, 1, stride=1, stride_axis=0)
                halo_bias[odd, group, spot, :] = turned[:, 0 : 2 * TILE]
                if odd == 0:
                    own_bias[group, spot, 0 : 2 * TILE] = turned[:, TILE : 3 * TILE]
                else:
                    own_bias[group, spot, 2 * TILE : 3 * TILE] = turned[:, 2 * TILE : 3 * TILE]


def swap_halves(part):
    tiles = [
        pltpu.roll(part[:, TILE * t : TILE * (t + 1)].astype(F32), SEG, 1).astype(BF16) for t in range(2)
    ]
    return jnp.concatenate(tiles, axis=1)


def query_code(own_codes, segment):
    lanes = lax.broadcasted_iota(jnp.int32, (SEG, 2 * TILE), 1)
    rows = lax.broadcasted_iota(jnp.int32, (SEG, 2 * TILE), 0)
    spread = jnp.broadcast_to(own_codes[0:1, :], (SEG, 2 * TILE))
    return jnp.sum(jnp.where(lanes == rows + SEG * segment, spread, 0.0), axis=1, keepdims=True)


def code_mask(codes, mine, low, high):
    lanes = lax.broadcasted_iota(jnp.int32, (SEG, codes.shape[1]), 1)
    agree = (jnp.broadcast_to(codes, (SEG, codes.shape[1])) == mine) & (lanes >= low) & (lanes < high)
    return jnp.where(agree, 0.0, NEG)


def half_scales():
    lanes = lax.broadcasted_iota(jnp.int32, (1, TILE), 1)
    scale = HEAD_SIZE ** (-0.5)
    low = jnp.where(lanes < HEAD_SIZE, scale, 0.0).astype(BF16)
    high = jnp.where(lanes < HEAD_SIZE, 0.0, scale).astype(BF16)
    return low, high


def stacked_queries(query, group):
    low, high = half_scales()
    return jnp.concatenate(
        [
            query[:, TILE * t : TILE * (t + 1)] * (low if (t < 2) == (group == 0) else high)
            for t in range(4)
        ],
        axis=0,
    )


def own_part(query, own, codes, own_bias, band, swapped, partial_ref, top_ref, total_ref):
    rows = own.shape[0]
    band[0:rows, :] = own
    band[rows:, :] = jnp.zeros((2 * TILE - rows, 2 * TILE), BF16)
    swapped[0:rows, :] = swap_halves(own)
    swapped[rows:, :] = jnp.zeros((2 * TILE - rows, 2 * TILE), BF16)
    for segment in range(3):
        width = 2 * TILE if segment == 2 else TILE
        first = (TILE, 2 * TILE, 0)[segment]
        mask = code_mask(codes[0:1, 0:width], query_code(codes, segment), 0, SEG * (segment + 1))
        for group in range(2):
            source = band if group == 0 else swapped
            left = stacked_queries(query[SEG * segment : SEG * (segment + 1), :], group)
            scores = lax.dot_general(
                left, source[0:width, 0:TILE], (((1,), (1,)), ((), ())), preferred_element_type=F32
            )
            base = 4 * SEG * (2 * segment + group)
            weights = []
            for block in range(4):
                spot = slice(SEG * block, SEG * (block + 1))
                s = scores[spot] + own_bias[group, spot, first : first + width] + mask
                top = jnp.max(s, axis=1, keepdims=True)
                e = jnp.exp(s - top)
                place = slice(base + SEG * block, base + SEG * (block + 1))
                top_ref[place, :] = jnp.broadcast_to(top, (SEG, TILE))
                total_ref[place, :] = jnp.broadcast_to(jnp.sum(e, axis=1, keepdims=True), (SEG, TILE))
                weights.append(e.astype(BF16))
            partial_ref[base : base + 4 * SEG, :] = jnp.dot(
                jnp.concatenate(weights, axis=0), source[0:width, TILE : 2 * TILE], preferred_element_type=F32
            )


def near_part(query_ref, near, codes, own_codes, halo_bias, partial_ref, top_ref, total_ref, band, swapped, mixed, heads_out):
    for target, rows in ((band, near), (swapped, swap_halves(near))):
        target[0:SEG, :] = jnp.zeros((SEG, 2 * TILE), BF16)
        target[SEG:, :] = rows
    lanes = lax.broadcasted_iota(jnp.int32, (1, TILE), 1)
    head_partial, head_top, head_total, head_left, head_code = heads_out
    for segment in range(3):
        start = TILE if segment == 2 else 0
        width = 2 * TILE - start
        mine = query_code(own_codes, segment)
        if segment == 0:
            head_code[...] = jnp.broadcast_to(mine, (SEG, TILE))
        mask = code_mask(codes[0:1, start:], mine, 0 if segment == 2 else SEG, width)
        results = []
        for group in range(2):
            source = band if group == 0 else swapped
            left = stacked_queries(query_ref[SEG * segment : SEG * (segment + 1), :], group)
            if segment == 0:
                turned = pltpu.roll(left.astype(F32), SEG, 1).astype(BF16) if group else left
                head_left[4 * SEG * group : 4 * SEG * (group + 1), :] = turned
            scores = lax.dot_general(
                left, source[start:, 0:TILE], (((1,), (1,)), ((), ())), preferred_element_type=F32
            )
            base = 4 * SEG * (2 * segment + group)
            weights = []
            olds = []
            shares = []
            for block in range(4):
                spot = slice(SEG * block, SEG * (block + 1))
                place = slice(base + SEG * block, base + SEG * (block + 1))
                s = scores[spot] + halo_bias[segment % 2, group, spot, 0:width] + mask
                old_top = top_ref[place, :]
                top = jnp.maximum(jnp.max(s, axis=1, keepdims=True), old_top)
                e = jnp.exp(s - jnp.concatenate([top] * (width // TILE), axis=1))
                old = jnp.exp(old_top - top)
                total = total_ref[place, :] * old + jnp.sum(e, axis=1, keepdims=True)
                weights.append(e.astype(BF16))
                if segment == 0:
                    head_top[place, :] = top
                    head_total[place, :] = total
                    olds.append(old)
                else:
                    share = 1.0 / total
                    shares.append(share)
                    olds.append(old * share)
            blended = jnp.dot(
                jnp.concatenate(weights, axis=0), source[start:, TILE : 2 * TILE], preferred_element_type=F32
            )
            for block in range(4):
                place = slice(base + SEG * block, base + SEG * (block + 1))
                fresh = blended[SEG * block : SEG * (block + 1)]
                before = partial_ref[place, :] * olds[block]
                if segment == 0:
                    head_partial[place, :] = fresh + before
                else:
                    results.append(fresh * shares[block] + before)
        if segment:
            store_heads(mixed, SEG * (segment - 1), results, lanes)


def store_heads(mixed, row, results, lanes):
    for tile in range(4):
        even, odd = (0, 4) if tile < 2 else (4, 0)
        mixed[row : row + SEG, TILE * tile : TILE * (tile + 1)] = jnp.where(
            lanes < HEAD_SIZE, results[even + tile], results[odd + tile]
        ).astype(BF16)


def far_part(far, codes, halo_bias, partial_ref, top_ref, total_ref, left_ref, code_ref, mixed):
    lanes = lax.broadcasted_iota(jnp.int32, (1, TILE), 1)
    scores = lax.dot_general(
        left_ref[...], far[:, 0:TILE], (((1,), (1,)), ((), ())), preferred_element_type=F32
    )
    values = far[:, TILE : 2 * TILE]
    both = jnp.concatenate([values, pltpu.roll(values.astype(F32), SEG, 1).astype(BF16)], axis=1)
    agree = jnp.broadcast_to(codes[0:1, 0:SEG], (SEG, SEG)) == code_ref[:, 0:SEG]
    mask = jnp.where(agree, 0.0, NEG)
    weights = []
    olds = []
    shares = []
    for block in range(8):
        spot = slice(SEG * (block % 4), SEG * (block % 4 + 1))
        place = slice(SEG * block, SEG * (block + 1))
        s = scores[place] + halo_bias[0, block // 4, spot, 0:SEG] + mask
        old_top = top_ref[place, :]
        top = jnp.maximum(jnp.max(s, axis=1, keepdims=True), old_top)
        e = jnp.exp(s - top[:, 0:SEG])
        old = jnp.exp(old_top - top)
        share = 1.0 / (total_ref[place, :] * old + jnp.sum(e, axis=1, keepdims=True))
        shares.append(share)
        olds.append(old * share)
        weights.append(e.astype(BF16))
    blended = jnp.dot(jnp.concatenate(weights, axis=0), both, preferred_element_type=F32)
    results = []
    for block in range(8):
        place = slice(SEG * block, SEG * (block + 1))
        side = slice(TILE * (block // 4), TILE * (block // 4 + 1))
        results.append(blended[place, side] * shares[block] + partial_ref[place, :] * olds[block])
    store_heads(mixed, 0, results, lanes)


def codes_of(packed_ref, row, turn):
    codes = packed_ref[row : row + 16, :].astype(F32)[0:8]
    return pltpu.roll(codes, turn, 1) if turn else codes


def before_one_kernel(
    query_hbm, key_w_hbm, value_w_hbm, packed_ref, table_ref, query_ref, weight_ref, halo_bias, partial_ref, top_ref,
    total_ref, own_bias, band, swapped, sems,
):
    rows = query_ref.shape[0]
    copy = pltpu.make_async_copy(query_hbm, query_ref, sems.at[0])
    copy.start()
    weight_copies = [
        pltpu.make_async_copy(key_w_hbm, weight_ref.at[:, 0:TILE], sems.at[1]),
        pltpu.make_async_copy(value_w_hbm, weight_ref.at[:, TILE : 2 * TILE], sems.at[2]),
    ]
    for weight_copy in weight_copies:
        weight_copy.start()
    fill_bias(table_ref, halo_bias, own_bias)
    own_codes = codes_of(packed_ref, rows, 2 * TILE - SEG)
    copy.wait()
    own_part(
        query_ref[...], packed_ref[0:rows, :], own_codes, own_bias, band, swapped, partial_ref, top_ref, total_ref
    )
    for weight_copy in weight_copies:
        weight_copy.wait()


def before_two_kernel(
    normed_ref, weight_ref, kv_ref, packed_ref, table_ref, query_ref, halo_bias, partial_ref, top_ref, total_ref,
    own_bias, band, swapped,
):
    rows = kv_ref.shape[0]
    query = jnp.dot(normed_ref[...], weight_ref[...], preferred_element_type=F32).astype(BF16)
    query_ref[...] = query
    fill_bias(table_ref, halo_bias, own_bias)
    own_codes = codes_of(packed_ref, rows, 2 * TILE - SEG)
    own_part(query, kv_ref[...], own_codes, own_bias, band, swapped, partial_ref, top_ref, total_ref)


def with_residual(partial, residual):
    mine = (lax.axis_index("tp") == 0).astype(F32)
    wide = residual.astype(F32)
    half = wide.shape[1]
    return (partial[:, 0:half] + wide * mine).astype(BF16), (partial[:, half:] + wide * (1.0 - mine)).astype(BF16)


def near_one_kernel(
    query_ref, near_ref, packed_ref, halo_bias, partial_ref, top_ref, total_ref, weight_ref, residual_ref,
    out_ref, head_partial, head_top, head_total, head_left, head_code, band, swapped, mixed,
):
    rows = query_ref.shape[0]
    near_part(
        query_ref, near_ref[0:rows, :], codes_of(near_ref, rows, 0), codes_of(packed_ref, rows, 2 * TILE - SEG),
        halo_bias, partial_ref, top_ref, total_ref, band, swapped, mixed,
        (head_partial, head_top, head_total, head_left, head_code),
    )
    partial = jnp.dot(mixed[...], weight_ref[...], preferred_element_type=F32)
    half = residual_ref.shape[1]
    out_ref[:, 0:half], out_ref[:, half:] = with_residual(partial, residual_ref[SEG:, :])


def near_two_kernel(
    query_ref, near_ref, near_codes_ref, packed_ref, halo_bias, partial_ref, top_ref, total_ref, weight_ref,
    out_ref, head_partial, head_top, head_total, head_left, head_code, band, swapped, mixed,
):
    rows = query_ref.shape[0]
    near_part(
        query_ref, near_ref[...], codes_of(near_codes_ref, rows, 0), codes_of(packed_ref, rows, 2 * TILE - SEG),
        halo_bias, partial_ref, top_ref, total_ref, band, swapped, mixed,
        (head_partial, head_top, head_total, head_left, head_code),
    )
    out_ref[...] = jnp.dot(mixed[...], weight_ref[...], preferred_element_type=F32).astype(BF16)


def far_one_kernel(
    far_ref, halo_bias, rest_ref, partial_ref, top_ref, total_ref, left_ref, code_ref, weight_ref, residual_ref,
    out_ref, mixed,
):
    out_ref[SEG:, :] = rest_ref[...]
    far_part(
        far_ref[0:SEG, :], codes_of(far_ref, SEG, 0), halo_bias, partial_ref, top_ref, total_ref, left_ref, code_ref, mixed
    )
    partial = jnp.dot(mixed[...], weight_ref[...], preferred_element_type=F32)
    half = residual_ref.shape[1]
    out_ref[0:SEG, 0:half], out_ref[0:SEG, half:] = with_residual(partial, residual_ref[0:SEG, :])


def far_two_kernel(
    far_ref, far_codes_ref, halo_bias, rest_ref, partial_ref, top_ref, total_ref, left_ref, code_ref, weight_ref,
    mine_ref, theirs_ref, mixed,
):
    half = mine_ref.shape[1]
    first = lax.axis_index("tp") == 0
    rest = rest_ref[...]
    mine_ref[SEG:, :] = jnp.where(first, rest[:, 0:half], rest[:, half:])
    theirs_ref[SEG:, :] = jnp.where(first, rest[:, half:], rest[:, 0:half])
    far_part(
        far_ref[...], codes_of(far_codes_ref, SEG, 0), halo_bias, partial_ref, top_ref, total_ref, left_ref, code_ref, mixed
    )
    partial = jnp.dot(mixed[...], weight_ref[...], preferred_element_type=F32).astype(BF16)
    mine_ref[0:SEG, :] = jnp.where(first, partial[:, 0:half], partial[:, half:])
    theirs_ref[0:SEG, :] = jnp.where(first, partial[:, half:], partial[:, 0:half])


def norm_kernel(both_ref, gain_ref, weight_ref, other_weight_ref, kv_ref, send_ref, tail_ref, normed_ref, share_ref):
    layer = both_ref[0] + both_ref[1]
    wide = layer.astype(F32)
    rows, channels = wide.shape
    scale = lax.rsqrt(jnp.mean(wide * wide, axis=1, keepdims=True) + EPS)
    normed = (wide * scale * gain_ref[...]).astype(BF16)
    send = jnp.dot(normed, other_weight_ref[...], preferred_element_type=F32).astype(BF16)
    send_ref[...] = send
    tail_ref[...] = send[rows - SEG :]
    kv_ref[...] = jnp.dot(normed, weight_ref[...], preferred_element_type=F32).astype(BF16)
    normed_ref[...] = normed
    half = channels // 2
    share_ref[...] = jnp.where(lax.axis_index("tp") == 0, layer[:, 0:half], layer[:, half:])


def last_kernel(both_ref, mine_ref, share_ref, out_hbm, out, sems):
    first = lax.axis_index("tp") == 0
    copies = []
    parts = sems.shape[0]
    rows = out.shape[0] // parts
    for part in range(parts):
        spot = slice(rows * part, rows * (part + 1))
        theirs = jnp.where(first, both_ref[1, spot, :], both_ref[0, spot, :])
        out[spot, :] = (
            share_ref[spot, :].astype(F32) + mine_ref[spot, :].astype(F32) + theirs.astype(F32)
        ).astype(BF16)
        copies.append(pltpu.make_async_copy(out.at[spot, :], out_hbm.at[spot, :], sems.at[part]))
        copies[-1].start()
    for copy in copies:
        copy.wait()


def call(kernel, outs, scratch, args, flops, mib=16, spaces=None, out_space=pltpu.VMEM):
    return pl.pallas_call(
        kernel,
        out_shape=outs,
        in_specs=[whole()] * len(args) if spaces is None else [pl.BlockSpec(memory_space=s) for s in spaces],
        out_specs=jax.tree.map(lambda _: pl.BlockSpec(memory_space=out_space), outs),
        scratch_shapes=scratch,
        compiler_params=params(mib),
        cost_estimate=cost(flops),
    )(*args)


def body(
    residual,
    query_first,
    key_first,
    value_first,
    documents,
    bias_first,
    out_first,
    norm_gain,
    query_w,
    key_w,
    value_w,
    bias_second,
    out_second,
):
    rows, half = residual.shape
    width = query_first.shape[1]
    channels = out_first.shape[1]
    docs = documents.reshape(1, rows)
    gain = norm_gain.reshape(1, channels)
    bands = [pltpu.VMEM((2 * TILE, 2 * TILE), BF16), pltpu.VMEM((2 * TILE, 2 * TILE), BF16)]
    before_scratch = [pltpu.VMEM((2, 4 * SEG, 3 * TILE), F32), *bands]
    near_scratch = [*bands, pltpu.VMEM((rows - SEG, width), BF16)]
    far_scratch = [pltpu.VMEM((SEG, width), BF16)]
    stats = shape(24 * SEG, TILE, dtype=F32)
    head_stats = shape(8 * SEG, TILE, dtype=F32)
    near_shapes = (
        shape(rows - SEG, channels),
        head_stats,
        head_stats,
        head_stats,
        shape(8 * SEG, TILE),
        shape(SEG, TILE, dtype=F32),
    )
    own_shapes = (shape(2, 2, 4 * SEG, 2 * TILE, dtype=F32), stats, stats, stats)
    packed, far_send = call(
        pack_kernel,
        (shape(rows + 16, 2 * TILE), shape(SEG + 16, 2 * TILE)),
        [pltpu.VMEM((8, 2 * TILE), F32), pltpu.VMEM((1, rows), jnp.int32), pltpu.SemaphoreType.DMA((7,))],
        tuple(pltpu.with_memory_space_constraint(x, pltpu.HBM) for x in (key_first, value_first, docs)),
        1 << 20,
        spaces=[pltpu.HBM] * 3,
    )
    near_one = from_behind(packed, 1)
    far_one = from_behind(far_send, 2)
    query_one, weights, *own_one = call(
        before_one_kernel,
        (shape(rows, width), shape(channels, 2 * TILE), *own_shapes),
        [*before_scratch, pltpu.SemaphoreType.DMA((3,))],
        (
            *(pltpu.with_memory_space_constraint(x, pltpu.HBM) for x in (query_first, key_w, value_w)),
            packed,
            bias_first,
        ),
        1 << 31,
        spaces=[pltpu.HBM] * 3 + [pltpu.VMEM] * 2,
    )
    other_weights = lax.ppermute(weights, "tp", [(0, 1), (1, 0)])
    rest_one = call(
        near_one_kernel,
        near_shapes,
        near_scratch,
        (query_one, near_one, packed, *own_one, out_first, residual),
        1 << 31,
    )
    sent_one = call(
        far_one_kernel,
        shape(rows, channels),
        far_scratch,
        (far_one, own_one[0], *rest_one, out_first, residual),
        1 << 31,
    )
    both_one = lax.all_gather(sent_one, "tp", axis=0)
    kv_two, send_two, tail_two, normed, share = call(
        norm_kernel,
        (
            shape(rows, 2 * TILE),
            shape(rows, 2 * TILE),
            shape(SEG, 2 * TILE),
            shape(rows, channels),
            shape(rows, half),
        ),
        [],
        (both_one, gain, weights, other_weights),
        1 << 30,
    )
    near_two = from_behind(send_two, 1, across=True)
    far_two = from_behind(tail_two, 2, across=True)
    query_two, *own_two = call(
        before_two_kernel,
        (shape(rows, width), *own_shapes),
        before_scratch,
        (normed, query_w, kv_two, packed, bias_second),
        1 << 31,
    )
    rest_two = call(
        near_two_kernel,
        near_shapes,
        near_scratch,
        (query_two, near_two, near_one, packed, *own_two, out_second),
        1 << 31,
    )
    mine_two, sent_two = call(
        far_two_kernel,
        (shape(rows, half), shape(rows, half)),
        far_scratch,
        (far_two, far_one, own_two[0], *rest_two, out_second),
        1 << 31,
    )
    both_two = lax.all_gather(sent_two, "tp", axis=0)
    return call(
        last_kernel,
        shape(rows, half),
        [pltpu.VMEM((rows, half), BF16), pltpu.SemaphoreType.DMA((4,))],
        (both_two, mine_two, share),
        1 << 20,
        out_space=pltpu.HBM,
    )


def solution(mesh):
    placed = (
        P("sp", "tp"),
        P("sp", "tp"),
        P("sp", "tp"),
        P("sp", "tp"),
        P("sp"),
        P("tp", None),
        P("tp", None),
        P(),
        P(None, "tp"),
        P(None, "tp"),
        P(None, "tp"),
        P("tp", None),
        P("tp", None),
    )
    return jax.shard_map(body, mesh=mesh, in_specs=placed, out_specs=P("sp", "tp"), check_vma=False)
```

```python
import jax
import jax.numpy as jnp
from jax import lax
from jax.experimental import pallas as pl
from jax.experimental.pallas import tpu as pltpu
from jax.sharding import PartitionSpec as P


HEAD_SIZE = 64
SEG = 64
EPS = 1e-06
TILE = 128
NEG = -1e30
F32 = jnp.float32
BF16 = jnp.bfloat16

GROUP_HEADS = ((0, 2, 5, 7), (1, 3, 4, 6))


def whole():
    return pl.BlockSpec(memory_space=pltpu.VMEM)


def params(mib):
    return pltpu.CompilerParams(vmem_limit_bytes=mib * 1024 * 1024)


def shape(*dims, dtype=BF16):
    return jax.ShapeDtypeStruct(dims, dtype)


def cost(flops, transcendentals=0, nbytes=1 << 20):
    return pl.CostEstimate(flops=flops, bytes_accessed=nbytes, transcendentals=transcendentals)


def from_behind(block, distance, across=False):
    devices = range(lax.axis_size("sp"))
    route = [(i - distance, i) for i in devices if i - distance in devices]
    if across:
        return lax.ppermute(
            block, ("sp", "tp"), [(2 * a + core, 2 * b + 1 - core) for a, b in route for core in range(2)]
        )
    return lax.ppermute(block, "sp", route)


def pack_kernel(key_hbm, value_hbm, doc_hbm, near_ref, far_ref, line, docs, sems):
    rows = key_hbm.shape[0]
    copies = [
        (doc_hbm, docs),
        *(
            (source.at[first : first + rows // 2, :], near_ref.at[first : first + rows // 2, lane : lane + TILE])
            for first in (0, rows // 2)
            for source, lane in ((key_hbm, 0), (value_hbm, TILE))
        ),
        (key_hbm.at[rows - SEG : rows, :], far_ref.at[0:SEG, 0:TILE]),
        (value_hbm.at[rows - SEG : rows, :], far_ref.at[0:SEG, TILE : 2 * TILE]),
    ]
    copies = [pltpu.make_async_copy(a, b, sems.at[i]) for i, (a, b) in enumerate(copies)]
    for copy in copies:
        copy.start()
    line[...] = jnp.zeros_like(line)
    copies[0].wait()
    codes = (docs[...] + 1).astype(F32)
    line[:, 0:rows] = jnp.broadcast_to(codes, (8, rows))
    flat = line[...]
    lanes = lax.broadcasted_iota(jnp.int32, flat.shape, 1)
    near = pltpu.roll(flat, SEG, 1)
    far = jnp.where(lanes < SEG, pltpu.roll(flat, 2 * TILE - (rows - SEG), 1), 0.0)
    near_ref[rows : rows + 8, :] = near.astype(BF16)
    far_ref[SEG : SEG + 8, :] = far.astype(BF16)
    for copy in copies[1:]:
        copy.wait()


def fill_bias(table_ref, halo_bias, own_bias):
    table = table_ref[:, 0 : 4 * TILE]
    last = table_ref[:, 4 * TILE : 4 * TILE + 1]
    lanes = lax.broadcasted_iota(jnp.int32, table.shape, 1)
    moved = jnp.where(lanes < 448, pltpu.roll(table, 448, 1), jnp.broadcast_to(last, table.shape))
    mirror = 127 - lax.broadcasted_iota(jnp.int32, (8, TILE), 1)
    pieces = [
        jnp.take_along_axis(moved[:, TILE * t : TILE * (t + 1)], mirror, axis=1)
        for t in (3, 2, 1, 0)
    ]
    line = jnp.concatenate(pieces, axis=1)
    for group in range(2):
        for block, head in enumerate(GROUP_HEADS[group]):
            rows = jnp.broadcast_to(line[head : head + 1, :], (SEG, 4 * TILE))
            spot = slice(SEG * block, SEG * (block + 1))
            for odd in range(2):
                turned = pltpu.roll(rows, 449 if odd == 0 else 1, 1, stride=1, stride_axis=0)
                halo_bias[odd, group, spot, :] = turned[:, 0 : 2 * TILE]
                if odd == 0:
                    own_bias[group, spot, 0 : 2 * TILE] = turned[:, TILE : 3 * TILE]
                else:
                    own_bias[group, spot, 2 * TILE : 3 * TILE] = turned[:, 2 * TILE : 3 * TILE]


def swap_halves(part):
    tiles = [
        pltpu.roll(part[:, TILE * t : TILE * (t + 1)].astype(F32), SEG, 1).astype(BF16) for t in range(2)
    ]
    return jnp.concatenate(tiles, axis=1)


def query_code(own_codes, segment):
    lanes = lax.broadcasted_iota(jnp.int32, (SEG, 2 * TILE), 1)
    rows = lax.broadcasted_iota(jnp.int32, (SEG, 2 * TILE), 0)
    spread = jnp.broadcast_to(own_codes[0:1, :], (SEG, 2 * TILE))
    return jnp.sum(jnp.where(lanes == rows + SEG * segment, spread, 0.0), axis=1, keepdims=True)


def code_mask(codes, mine, low, high):
    lanes = lax.broadcasted_iota(jnp.int32, (SEG, codes.shape[1]), 1)
    agree = (jnp.broadcast_to(codes, (SEG, codes.shape[1])) == mine) & (lanes >= low) & (lanes < high)
    return jnp.where(agree, 0.0, NEG)


def half_scales():
    lanes = lax.broadcasted_iota(jnp.int32, (1, TILE), 1)
    scale = HEAD_SIZE ** (-0.5)
    low = jnp.where(lanes < HEAD_SIZE, scale, 0.0).astype(BF16)
    high = jnp.where(lanes < HEAD_SIZE, 0.0, scale).astype(BF16)
    return low, high


def stacked_queries(query, group):
    low, high = half_scales()
    return jnp.concatenate(
        [
            query[:, TILE * t : TILE * (t + 1)] * (low if (t < 2) == (group == 0) else high)
            for t in range(4)
        ],
        axis=0,
    )


def own_part(query, own, codes, own_bias, band, swapped, partial_ref, top_ref, total_ref):
    rows = own.shape[0]
    band[0:rows, :] = own
    band[rows:, :] = jnp.zeros((2 * TILE - rows, 2 * TILE), BF16)
    swapped[0:rows, :] = swap_halves(own)
    swapped[rows:, :] = jnp.zeros((2 * TILE - rows, 2 * TILE), BF16)
    for segment in range(3):
        width = 2 * TILE if segment == 2 else TILE
        first = (TILE, 2 * TILE, 0)[segment]
        mask = code_mask(codes[0:1, 0:width], query_code(codes, segment), 0, SEG * (segment + 1))
        for group in range(2):
            source = band if group == 0 else swapped
            left = stacked_queries(query[SEG * segment : SEG * (segment + 1), :], group)
            scores = lax.dot_general(
                left, source[0:width, 0:TILE], (((1,), (1,)), ((), ())), preferred_element_type=F32
            )
            base = 4 * SEG * (2 * segment + group)
            weights = []
            for block in range(4):
                spot = slice(SEG * block, SEG * (block + 1))
                s = scores[spot] + own_bias[group, spot, first : first + width] + mask
                top = jnp.max(s, axis=1, keepdims=True)
                e = jnp.exp(s - top)
                place = slice(base + SEG * block, base + SEG * (block + 1))
                top_ref[place, :] = jnp.broadcast_to(top, (SEG, TILE))
                total_ref[place, :] = jnp.broadcast_to(jnp.sum(e, axis=1, keepdims=True), (SEG, TILE))
                weights.append(e.astype(BF16))
            partial_ref[base : base + 4 * SEG, :] = jnp.dot(
                jnp.concatenate(weights, axis=0), source[0:width, TILE : 2 * TILE], preferred_element_type=F32
            )


def near_part(query_ref, near, codes, own_codes, halo_bias, partial_ref, top_ref, total_ref, band, swapped, mixed, heads_out):
    for target, rows in ((band, near), (swapped, swap_halves(near))):
        target[0:SEG, :] = jnp.zeros((SEG, 2 * TILE), BF16)
        target[SEG:, :] = rows
    lanes = lax.broadcasted_iota(jnp.int32, (1, TILE), 1)
    head_partial, head_top, head_total, head_left, head_code = heads_out
    for segment in range(3):
        start = TILE if segment == 2 else 0
        width = 2 * TILE - start
        mine = query_code(own_codes, segment)
        if segment == 0:
            head_code[...] = jnp.broadcast_to(mine, (SEG, TILE))
        mask = code_mask(codes[0:1, start:], mine, 0 if segment == 2 else SEG, width)
        results = []
        for group in range(2):
            source = band if group == 0 else swapped
            left = stacked_queries(query_ref[SEG * segment : SEG * (segment + 1), :], group)
            if segment == 0:
                turned = pltpu.roll(left.astype(F32), SEG, 1).astype(BF16) if group else left
                head_left[4 * SEG * group : 4 * SEG * (group + 1), :] = turned
            scores = lax.dot_general(
                left, source[start:, 0:TILE], (((1,), (1,)), ((), ())), preferred_element_type=F32
            )
            base = 4 * SEG * (2 * segment + group)
            weights = []
            olds = []
            shares = []
            for block in range(4):
                spot = slice(SEG * block, SEG * (block + 1))
                place = slice(base + SEG * block, base + SEG * (block + 1))
                s = scores[spot] + halo_bias[segment % 2, group, spot, 0:width] + mask
                old_top = top_ref[place, :]
                top = jnp.maximum(jnp.max(s, axis=1, keepdims=True), old_top)
                e = jnp.exp(s - jnp.concatenate([top] * (width // TILE), axis=1))
                old = jnp.exp(old_top - top)
                total = total_ref[place, :] * old + jnp.sum(e, axis=1, keepdims=True)
                weights.append(e.astype(BF16))
                if segment == 0:
                    head_top[place, :] = top
                    head_total[place, :] = total
                    olds.append(old)
                else:
                    share = 1.0 / total
                    shares.append(share)
                    olds.append(old * share)
            blended = jnp.dot(
                jnp.concatenate(weights, axis=0), source[start:, TILE : 2 * TILE], preferred_element_type=F32
            )
            for block in range(4):
                place = slice(base + SEG * block, base + SEG * (block + 1))
                fresh = blended[SEG * block : SEG * (block + 1)]
                before = partial_ref[place, :] * olds[block]
                if segment == 0:
                    head_partial[place, :] = fresh + before
                else:
                    results.append(fresh * shares[block] + before)
        if segment:
            store_heads(mixed, SEG * (segment - 1), results, lanes)


def store_heads(mixed, row, results, lanes):
    for tile in range(4):
        even, odd = (0, 4) if tile < 2 else (4, 0)
        mixed[row : row + SEG, TILE * tile : TILE * (tile + 1)] = jnp.where(
            lanes < HEAD_SIZE, results[even + tile], results[odd + tile]
        ).astype(BF16)


def far_part(far, codes, halo_bias, partial_ref, top_ref, total_ref, left_ref, code_ref, mixed):
    lanes = lax.broadcasted_iota(jnp.int32, (1, TILE), 1)
    scores = lax.dot_general(
        left_ref[...], far[:, 0:TILE], (((1,), (1,)), ((), ())), preferred_element_type=F32
    )
    values = far[:, TILE : 2 * TILE]
    both = jnp.concatenate([values, pltpu.roll(values.astype(F32), SEG, 1).astype(BF16)], axis=1)
    agree = jnp.broadcast_to(codes[0:1, 0:SEG], (SEG, SEG)) == code_ref[:, 0:SEG]
    mask = jnp.where(agree, 0.0, NEG)
    weights = []
    olds = []
    shares = []
    for block in range(8):
        spot = slice(SEG * (block % 4), SEG * (block % 4 + 1))
        place = slice(SEG * block, SEG * (block + 1))
        s = scores[place] + halo_bias[0, block // 4, spot, 0:SEG] + mask
        old_top = top_ref[place, :]
        top = jnp.maximum(jnp.max(s, axis=1, keepdims=True), old_top)
        e = jnp.exp(s - top[:, 0:SEG])
        old = jnp.exp(old_top - top)
        share = 1.0 / (total_ref[place, :] * old + jnp.sum(e, axis=1, keepdims=True))
        shares.append(share)
        olds.append(old * share)
        weights.append(e.astype(BF16))
    blended = jnp.dot(jnp.concatenate(weights, axis=0), both, preferred_element_type=F32)
    results = []
    for block in range(8):
        place = slice(SEG * block, SEG * (block + 1))
        side = slice(TILE * (block // 4), TILE * (block // 4 + 1))
        results.append(blended[place, side] * shares[block] + partial_ref[place, :] * olds[block])
    store_heads(mixed, 0, results, lanes)


def codes_of(packed_ref, row, turn):
    codes = packed_ref[row : row + 8, :].astype(F32)
    return pltpu.roll(codes, turn, 1) if turn else codes


def before_one_kernel(
    query_hbm, key_w_hbm, value_w_hbm, packed_ref, table_ref, query_ref, weight_ref, halo_bias, partial_ref, top_ref,
    total_ref, own_bias, band, swapped, sems,
):
    rows = query_ref.shape[0]
    copy = pltpu.make_async_copy(query_hbm, query_ref, sems.at[0])
    copy.start()
    weight_copies = [
        pltpu.make_async_copy(key_w_hbm, weight_ref.at[:, 0:TILE], sems.at[1]),
        pltpu.make_async_copy(value_w_hbm, weight_ref.at[:, TILE : 2 * TILE], sems.at[2]),
    ]
    for weight_copy in weight_copies:
        weight_copy.start()
    fill_bias(table_ref, halo_bias, own_bias)
    own_codes = codes_of(packed_ref, rows, 2 * TILE - SEG)
    copy.wait()
    own_part(
        query_ref[...], packed_ref[0:rows, :], own_codes, own_bias, band, swapped, partial_ref, top_ref, total_ref
    )
    for weight_copy in weight_copies:
        weight_copy.wait()


def before_two_kernel(
    normed_ref, weight_ref, kv_weight_ref, packed_ref, table_ref, query_ref, halo_bias, partial_ref, top_ref, total_ref,
    own_bias, band, swapped,
):
    rows = normed_ref.shape[0]
    own = jnp.dot(normed_ref[...], kv_weight_ref[...], preferred_element_type=F32).astype(BF16)
    query = jnp.dot(normed_ref[...], weight_ref[...], preferred_element_type=F32).astype(BF16)
    query_ref[...] = query
    fill_bias(table_ref, halo_bias, own_bias)
    own_codes = codes_of(packed_ref, rows, 2 * TILE - SEG)
    own_part(query, own, own_codes, own_bias, band, swapped, partial_ref, top_ref, total_ref)


def with_residual(partial, residual):
    mine = (lax.axis_index("tp") == 0).astype(F32)
    wide = residual.astype(F32)
    half = wide.shape[1]
    return (partial[:, 0:half] + wide * mine).astype(BF16), (partial[:, half:] + wide * (1.0 - mine)).astype(BF16)


def near_one_kernel(
    query_ref, near_ref, packed_ref, halo_bias, partial_ref, top_ref, total_ref, weight_ref, residual_ref,
    out_ref, head_partial, head_top, head_total, head_left, head_code, band, swapped, mixed,
):
    rows = query_ref.shape[0]
    near_part(
        query_ref, near_ref[0:rows, :], codes_of(near_ref, rows, 0), codes_of(packed_ref, rows, 2 * TILE - SEG),
        halo_bias, partial_ref, top_ref, total_ref, band, swapped, mixed,
        (head_partial, head_top, head_total, head_left, head_code),
    )
    partial = jnp.dot(mixed[...], weight_ref[...], preferred_element_type=F32)
    half = residual_ref.shape[1]
    out_ref[:, 0:half], out_ref[:, half:] = with_residual(partial, residual_ref[SEG:, :])


def near_two_kernel(
    query_ref, near_ref, near_codes_ref, packed_ref, halo_bias, partial_ref, top_ref, total_ref, weight_ref,
    out_ref, head_partial, head_top, head_total, head_left, head_code, band, swapped, mixed,
):
    rows = query_ref.shape[0]
    near_part(
        query_ref, near_ref[...], codes_of(near_codes_ref, rows, 0), codes_of(packed_ref, rows, 2 * TILE - SEG),
        halo_bias, partial_ref, top_ref, total_ref, band, swapped, mixed,
        (head_partial, head_top, head_total, head_left, head_code),
    )
    out_ref[...] = jnp.dot(mixed[...], weight_ref[...], preferred_element_type=F32).astype(BF16)


def far_one_kernel(
    far_ref, halo_bias, rest_ref, partial_ref, top_ref, total_ref, left_ref, code_ref, weight_ref, residual_ref,
    out_ref, mixed,
):
    out_ref[SEG:, :] = rest_ref[...]
    far_part(
        far_ref[0:SEG, :], codes_of(far_ref, SEG, 0), halo_bias, partial_ref, top_ref, total_ref, left_ref, code_ref, mixed
    )
    partial = jnp.dot(mixed[...], weight_ref[...], preferred_element_type=F32)
    half = residual_ref.shape[1]
    out_ref[0:SEG, 0:half], out_ref[0:SEG, half:] = with_residual(partial, residual_ref[0:SEG, :])


def far_two_kernel(
    far_ref, far_codes_ref, halo_bias, rest_ref, partial_ref, top_ref, total_ref, left_ref, code_ref, weight_ref,
    mine_ref, theirs_ref, mixed,
):
    half = mine_ref.shape[1]
    first = lax.axis_index("tp") == 0
    rest = rest_ref[...]
    mine_ref[SEG:, :] = jnp.where(first, rest[:, 0:half], rest[:, half:])
    theirs_ref[SEG:, :] = jnp.where(first, rest[:, half:], rest[:, 0:half])
    far_part(
        far_ref[...], codes_of(far_codes_ref, SEG, 0), halo_bias, partial_ref, top_ref, total_ref, left_ref, code_ref, mixed
    )
    partial = jnp.dot(mixed[...], weight_ref[...], preferred_element_type=F32).astype(BF16)
    mine_ref[0:SEG, :] = jnp.where(first, partial[:, 0:half], partial[:, half:])
    theirs_ref[0:SEG, :] = jnp.where(first, partial[:, half:], partial[:, 0:half])


def norm_kernel(both_ref, gain_ref, other_weight_ref, send_ref, tail_ref, normed_ref, share_ref):
    layer = both_ref[0] + both_ref[1]
    wide = layer.astype(F32)
    rows, channels = wide.shape
    scale = lax.rsqrt(jnp.mean(wide * wide, axis=1, keepdims=True) + EPS)
    normed = (wide * scale * gain_ref[...]).astype(BF16)
    send = jnp.dot(normed, other_weight_ref[...], preferred_element_type=F32).astype(BF16)
    send_ref[...] = send
    tail_ref[...] = send[rows - SEG :]
    normed_ref[...] = normed
    half = channels // 2
    share_ref[...] = jnp.where(lax.axis_index("tp") == 0, layer[:, 0:half], layer[:, half:])


def last_kernel(both_ref, mine_ref, share_ref, out_hbm, out, sems):
    first = lax.axis_index("tp") == 0
    copies = []
    parts = sems.shape[0]
    rows = out.shape[0] // parts
    for part in range(parts):
        spot = slice(rows * part, rows * (part + 1))
        theirs = jnp.where(first, both_ref[1, spot, :], both_ref[0, spot, :])
        out[spot, :] = (
            share_ref[spot, :].astype(F32) + mine_ref[spot, :].astype(F32) + theirs.astype(F32)
        ).astype(BF16)
        copies.append(pltpu.make_async_copy(out.at[spot, :], out_hbm.at[spot, :], sems.at[part]))
        copies[-1].start()
    for copy in copies:
        copy.wait()


def call(kernel, outs, scratch, args, flops, mib=16, spaces=None, out_space=pltpu.VMEM):
    return pl.pallas_call(
        kernel,
        out_shape=outs,
        in_specs=[whole()] * len(args) if spaces is None else [pl.BlockSpec(memory_space=s) for s in spaces],
        out_specs=jax.tree.map(lambda _: pl.BlockSpec(memory_space=out_space), outs),
        scratch_shapes=scratch,
        compiler_params=params(mib),
        cost_estimate=cost(flops),
    )(*args)


def body(
    residual,
    query_first,
    key_first,
    value_first,
    documents,
    bias_first,
    out_first,
    norm_gain,
    query_w,
    key_w,
    value_w,
    bias_second,
    out_second,
):
    rows, half = residual.shape
    width = query_first.shape[1]
    channels = out_first.shape[1]
    docs = documents.reshape(1, rows)
    gain = norm_gain.reshape(1, channels)
    bands = [pltpu.VMEM((2 * TILE, 2 * TILE), BF16), pltpu.VMEM((2 * TILE, 2 * TILE), BF16)]
    before_scratch = [pltpu.VMEM((2, 4 * SEG, 3 * TILE), F32), *bands]
    near_scratch = [*bands, pltpu.VMEM((rows - SEG, width), BF16)]
    far_scratch = [pltpu.VMEM((SEG, width), BF16)]
    stats = shape(24 * SEG, TILE, dtype=F32)
    head_stats = shape(8 * SEG, TILE, dtype=F32)
    near_shapes = (
        shape(rows - SEG, channels),
        head_stats,
        head_stats,
        head_stats,
        shape(8 * SEG, TILE),
        shape(SEG, TILE, dtype=F32),
    )
    own_shapes = (shape(2, 2, 4 * SEG, 2 * TILE, dtype=F32), stats, stats, stats)
    packed, far_send = call(
        pack_kernel,
        (shape(rows + 8, 2 * TILE), shape(SEG + 8, 2 * TILE)),
        [pltpu.VMEM((8, 2 * TILE), F32), pltpu.VMEM((1, rows), jnp.int32), pltpu.SemaphoreType.DMA((7,))],
        tuple(pltpu.with_memory_space_constraint(x, pltpu.HBM) for x in (key_first, value_first, docs)),
        1 << 20,
        spaces=[pltpu.HBM] * 3,
    )
    near_one = from_behind(packed, 1)
    far_one = from_behind(far_send, 2)
    query_one, weights, *own_one = call(
        before_one_kernel,
        (shape(rows, width), shape(channels, 2 * TILE), *own_shapes),
        [*before_scratch, pltpu.SemaphoreType.DMA((3,))],
        (
            *(pltpu.with_memory_space_constraint(x, pltpu.HBM) for x in (query_first, key_w, value_w)),
            packed,
            bias_first,
        ),
        1 << 31,
        spaces=[pltpu.HBM] * 3 + [pltpu.VMEM] * 2,
    )
    other_weights = lax.ppermute(weights, "tp", [(0, 1), (1, 0)])
    rest_one = call(
        near_one_kernel,
        near_shapes,
        near_scratch,
        (query_one, near_one, packed, *own_one, out_first, residual),
        1 << 31,
    )
    sent_one = call(
        far_one_kernel,
        shape(rows, channels),
        far_scratch,
        (far_one, own_one[0], *rest_one, out_first, residual),
        1 << 31,
    )
    both_one = lax.all_gather(sent_one, "tp", axis=0)
    send_two, tail_two, normed, share = call(
        norm_kernel,
        (
            shape(rows, 2 * TILE),
            shape(SEG, 2 * TILE),
            shape(rows, channels),
            shape(rows, half),
        ),
        [],
        (both_one, gain, other_weights),
        1 << 30,
    )
    near_two = from_behind(send_two, 1, across=True)
    far_two = from_behind(tail_two, 2, across=True)
    query_two, *own_two = call(
        before_two_kernel,
        (shape(rows, width), *own_shapes),
        before_scratch,
        (normed, query_w, weights, packed, bias_second),
        1 << 31,
    )
    rest_two = call(
        near_two_kernel,
        near_shapes,
        near_scratch,
        (query_two, near_two, near_one, packed, *own_two, out_second),
        1 << 31,
    )
    mine_two, sent_two = call(
        far_two_kernel,
        (shape(rows, half), shape(rows, half)),
        far_scratch,
        (far_two, far_one, own_two[0], *rest_two, out_second),
        1 << 31,
    )
    both_two = lax.all_gather(sent_two, "tp", axis=0)
    return call(
        last_kernel,
        shape(rows, half),
        [pltpu.VMEM((rows, half), BF16), pltpu.SemaphoreType.DMA((4,))],
        (both_two, mine_two, share),
        1 << 20,
        out_space=pltpu.HBM,
    )


def solution(mesh):
    placed = (
        P("sp", "tp"),
        P("sp", "tp"),
        P("sp", "tp"),
        P("sp", "tp"),
        P("sp"),
        P("tp", None),
        P("tp", None),
        P(),
        P(None, "tp"),
        P(None, "tp"),
        P(None, "tp"),
        P("tp", None),
        P("tp", None),
    )
    return jax.shard_map(body, mesh=mesh, in_specs=placed, out_specs=P("sp", "tp"), check_vma=False)
```

```python
import jax
import jax.numpy as jnp
from jax import lax
from jax.experimental import pallas as pl
from jax.experimental.pallas import tpu as pltpu
from jax.sharding import PartitionSpec as P


HEAD_SIZE = 64
SEG = 64
EPS = 1e-06
TILE = 128
NEG = -1e30
F32 = jnp.float32
BF16 = jnp.bfloat16

GROUP_HEADS = ((0, 2, 5, 7), (1, 3, 4, 6))


def whole():
    return pl.BlockSpec(memory_space=pltpu.VMEM)


def params(mib):
    return pltpu.CompilerParams(vmem_limit_bytes=mib * 1024 * 1024)


def shape(*dims, dtype=BF16):
    return jax.ShapeDtypeStruct(dims, dtype)


def cost(flops, transcendentals=0, nbytes=1 << 20):
    return pl.CostEstimate(flops=flops, bytes_accessed=nbytes, transcendentals=transcendentals)


def from_behind(block, distance, across=False):
    devices = range(lax.axis_size("sp"))
    route = [(i - distance, i) for i in devices if i - distance in devices]
    if across:
        return lax.ppermute(
            block, ("sp", "tp"), [(2 * a + core, 2 * b + 1 - core) for a, b in route for core in range(2)]
        )
    return lax.ppermute(block, "sp", route)


def pack_kernel(key_hbm, value_hbm, doc_hbm, near_ref, far_ref, line, docs, sems):
    rows = key_hbm.shape[0]
    copies = [
        (doc_hbm, docs),
        *(
            (source.at[first : first + rows // 2, :], near_ref.at[first : first + rows // 2, lane : lane + TILE])
            for first in (0, rows // 2)
            for source, lane in ((key_hbm, 0), (value_hbm, TILE))
        ),
        (key_hbm.at[rows - SEG : rows, :], far_ref.at[0:SEG, 0:TILE]),
        (value_hbm.at[rows - SEG : rows, :], far_ref.at[0:SEG, TILE : 2 * TILE]),
    ]
    copies = [pltpu.make_async_copy(a, b, sems.at[i]) for i, (a, b) in enumerate(copies)]
    for copy in copies:
        copy.start()
    line[...] = jnp.zeros_like(line)
    copies[0].wait()
    codes = (docs[...] + 1).astype(F32)
    line[:, 0:rows] = jnp.broadcast_to(codes, (8, rows))
    flat = line[...]
    lanes = lax.broadcasted_iota(jnp.int32, flat.shape, 1)
    near = pltpu.roll(flat, SEG, 1)
    far = jnp.where(lanes < SEG, pltpu.roll(flat, 2 * TILE - (rows - SEG), 1), 0.0)
    near_ref[rows : rows + 8, :] = near.astype(BF16)
    far_ref[SEG : SEG + 8, :] = far.astype(BF16)
    for copy in copies[1:]:
        copy.wait()


def fill_bias(table_ref, halo_bias, own_bias):
    table = table_ref[:, 0 : 4 * TILE]
    last = table_ref[:, 4 * TILE : 4 * TILE + 1]
    lanes = lax.broadcasted_iota(jnp.int32, table.shape, 1)
    moved = jnp.where(lanes < 448, pltpu.roll(table, 448, 1), jnp.broadcast_to(last, table.shape))
    mirror = 127 - lax.broadcasted_iota(jnp.int32, (8, TILE), 1)
    pieces = [
        jnp.take_along_axis(moved[:, TILE * t : TILE * (t + 1)], mirror, axis=1)
        for t in (3, 2, 1, 0)
    ]
    line = jnp.concatenate(pieces, axis=1)
    for group in range(2):
        for block, head in enumerate(GROUP_HEADS[group]):
            rows = jnp.broadcast_to(line[head : head + 1, :], (SEG, 4 * TILE))
            spot = slice(SEG * block, SEG * (block + 1))
            for odd in range(2):
                turned = pltpu.roll(rows, 449 if odd == 0 else 1, 1, stride=1, stride_axis=0)
                halo_bias[odd, group, spot, :] = turned[:, 0 : 2 * TILE]
                if odd == 0:
                    own_bias[group, spot, 0 : 2 * TILE] = turned[:, TILE : 3 * TILE]
                else:
                    own_bias[group, spot, 2 * TILE : 3 * TILE] = turned[:, 2 * TILE : 3 * TILE]


def swap_halves(part):
    tiles = [
        pltpu.roll(part[:, TILE * t : TILE * (t + 1)].astype(F32), SEG, 1).astype(BF16) for t in range(2)
    ]
    return jnp.concatenate(tiles, axis=1)


def query_code(own_codes, segment):
    lanes = lax.broadcasted_iota(jnp.int32, (SEG, 2 * TILE), 1)
    rows = lax.broadcasted_iota(jnp.int32, (SEG, 2 * TILE), 0)
    spread = jnp.broadcast_to(own_codes[0:1, :], (SEG, 2 * TILE))
    return jnp.sum(jnp.where(lanes == rows + SEG * segment, spread, 0.0), axis=1, keepdims=True)


def code_mask(codes, mine, low, high):
    lanes = lax.broadcasted_iota(jnp.int32, (SEG, codes.shape[1]), 1)
    agree = (jnp.broadcast_to(codes, (SEG, codes.shape[1])) == mine) & (lanes >= low) & (lanes < high)
    return jnp.where(agree, 0.0, NEG)


def half_scales():
    lanes = lax.broadcasted_iota(jnp.int32, (1, TILE), 1)
    scale = HEAD_SIZE ** (-0.5)
    low = jnp.where(lanes < HEAD_SIZE, scale, 0.0).astype(BF16)
    high = jnp.where(lanes < HEAD_SIZE, 0.0, scale).astype(BF16)
    return low, high


def stacked_queries(query, group):
    low, high = half_scales()
    return jnp.concatenate(
        [
            query[:, TILE * t : TILE * (t + 1)] * (low if (t < 2) == (group == 0) else high)
            for t in range(4)
        ],
        axis=0,
    )


def own_part(query, own, codes, own_bias, band, swapped, partial_ref, top_ref, total_ref):
    rows = own.shape[0]
    band[0:rows, :] = own
    band[rows:, :] = jnp.zeros((2 * TILE - rows, 2 * TILE), BF16)
    swapped[0:rows, :] = swap_halves(own)
    swapped[rows:, :] = jnp.zeros((2 * TILE - rows, 2 * TILE), BF16)
    for segment in range(3):
        width = 2 * TILE if segment == 2 else TILE
        first = (TILE, 2 * TILE, 0)[segment]
        mask = code_mask(codes[0:1, 0:width], query_code(codes, segment), 0, SEG * (segment + 1))
        for group in range(2):
            source = band if group == 0 else swapped
            left = stacked_queries(query[SEG * segment : SEG * (segment + 1), :], group)
            scores = lax.dot_general(
                left, source[0:width, 0:TILE], (((1,), (1,)), ((), ())), preferred_element_type=F32
            )
            base = 4 * SEG * (2 * segment + group)
            weights = []
            for block in range(4):
                spot = slice(SEG * block, SEG * (block + 1))
                s = scores[spot] + own_bias[group, spot, first : first + width] + mask
                top = jnp.max(s, axis=1, keepdims=True)
                e = jnp.exp(s - top)
                place = slice(base + SEG * block, base + SEG * (block + 1))
                top_ref[place, :] = jnp.broadcast_to(top, (SEG, TILE))
                total_ref[place, :] = jnp.broadcast_to(jnp.sum(e, axis=1, keepdims=True), (SEG, TILE))
                weights.append(e.astype(BF16))
            partial_ref[base : base + 4 * SEG, :] = jnp.dot(
                jnp.concatenate(weights, axis=0), source[0:width, TILE : 2 * TILE], preferred_element_type=F32
            )


def near_part(query_ref, near, codes, own_codes, halo_bias, partial_ref, top_ref, total_ref, band, swapped, mixed, heads_out):
    for target, rows in ((band, near), (swapped, swap_halves(near))):
        target[0:SEG, :] = jnp.zeros((SEG, 2 * TILE), BF16)
        target[SEG:, :] = rows
    lanes = lax.broadcasted_iota(jnp.int32, (1, TILE), 1)
    head_partial, head_top, head_total, head_left, head_code = heads_out
    for segment in range(3):
        start = TILE if segment == 2 else 0
        width = 2 * TILE - start
        mine = query_code(own_codes, segment)
        if segment == 0:
            head_code[...] = jnp.broadcast_to(mine, (SEG, TILE))
        mask = code_mask(codes[0:1, start:], mine, 0 if segment == 2 else SEG, width)
        results = []
        for group in range(2):
            source = band if group == 0 else swapped
            left = stacked_queries(query_ref[SEG * segment : SEG * (segment + 1), :], group)
            if segment == 0:
                turned = pltpu.roll(left.astype(F32), SEG, 1).astype(BF16) if group else left
                head_left[4 * SEG * group : 4 * SEG * (group + 1), :] = turned
            scores = lax.dot_general(
                left, source[start:, 0:TILE], (((1,), (1,)), ((), ())), preferred_element_type=F32
            )
            base = 4 * SEG * (2 * segment + group)
            weights = []
            olds = []
            shares = []
            for block in range(4):
                spot = slice(SEG * block, SEG * (block + 1))
                place = slice(base + SEG * block, base + SEG * (block + 1))
                s = scores[spot] + halo_bias[segment % 2, group, spot, 0:width] + mask
                old_top = top_ref[place, :]
                top = jnp.maximum(jnp.max(s, axis=1, keepdims=True), old_top)
                e = jnp.exp(s - jnp.concatenate([top] * (width // TILE), axis=1))
                old = jnp.exp(old_top - top)
                total = total_ref[place, :] * old + jnp.sum(e, axis=1, keepdims=True)
                weights.append(e.astype(BF16))
                if segment == 0:
                    head_top[place, :] = top
                    head_total[place, :] = total
                    olds.append(old)
                else:
                    share = 1.0 / total
                    shares.append(share)
                    olds.append(old * share)
            blended = jnp.dot(
                jnp.concatenate(weights, axis=0), source[start:, TILE : 2 * TILE], preferred_element_type=F32
            )
            for block in range(4):
                place = slice(base + SEG * block, base + SEG * (block + 1))
                fresh = blended[SEG * block : SEG * (block + 1)]
                before = partial_ref[place, :] * olds[block]
                if segment == 0:
                    head_partial[place, :] = fresh + before
                else:
                    results.append(fresh * shares[block] + before)
        if segment:
            store_heads(mixed, SEG * (segment - 1), results, lanes)


def store_heads(mixed, row, results, lanes):
    for tile in range(4):
        even, odd = (0, 4) if tile < 2 else (4, 0)
        mixed[row : row + SEG, TILE * tile : TILE * (tile + 1)] = jnp.where(
            lanes < HEAD_SIZE, results[even + tile], results[odd + tile]
        ).astype(BF16)


def far_part(far, codes, halo_bias, partial_ref, top_ref, total_ref, left_ref, code_ref, mixed):
    lanes = lax.broadcasted_iota(jnp.int32, (1, TILE), 1)
    scores = lax.dot_general(
        left_ref[...], far[:, 0:TILE], (((1,), (1,)), ((), ())), preferred_element_type=F32
    )
    values = far[:, TILE : 2 * TILE]
    both = jnp.concatenate([values, pltpu.roll(values.astype(F32), SEG, 1).astype(BF16)], axis=1)
    agree = jnp.broadcast_to(codes[0:1, 0:SEG], (SEG, SEG)) == code_ref[:, 0:SEG]
    mask = jnp.where(agree, 0.0, NEG)
    weights = []
    olds = []
    shares = []
    for block in range(8):
        spot = slice(SEG * (block % 4), SEG * (block % 4 + 1))
        place = slice(SEG * block, SEG * (block + 1))
        s = scores[place] + halo_bias[0, block // 4, spot, 0:SEG] + mask
        old_top = top_ref[place, :]
        top = jnp.maximum(jnp.max(s, axis=1, keepdims=True), old_top)
        e = jnp.exp(s - top[:, 0:SEG])
        old = jnp.exp(old_top - top)
        shares.append(1.0 / (total_ref[place, :] * old + jnp.sum(e, axis=1, keepdims=True)))
        olds.append(old)
        weights.append(e.astype(BF16))
    blended = jnp.dot(jnp.concatenate(weights, axis=0), both, preferred_element_type=F32)
    results = []
    for block in range(8):
        place = slice(SEG * block, SEG * (block + 1))
        side = slice(TILE * (block // 4), TILE * (block // 4 + 1))
        results.append((blended[place, side] + partial_ref[place, :] * olds[block]) * shares[block])
    store_heads(mixed, 0, results, lanes)


def codes_of(packed_ref, row, turn):
    codes = packed_ref[row : row + 8, :].astype(F32)
    return pltpu.roll(codes, turn, 1) if turn else codes


def before_one_kernel(
    query_hbm, key_w_hbm, value_w_hbm, packed_ref, table_ref, query_ref, weight_ref, halo_bias, partial_ref, top_ref,
    total_ref, own_bias, band, swapped, sems,
):
    rows = query_ref.shape[0]
    copy = pltpu.make_async_copy(query_hbm, query_ref, sems.at[0])
    copy.start()
    weight_copies = [
        pltpu.make_async_copy(key_w_hbm, weight_ref.at[:, 0:TILE], sems.at[1]),
        pltpu.make_async_copy(value_w_hbm, weight_ref.at[:, TILE : 2 * TILE], sems.at[2]),
    ]
    for weight_copy in weight_copies:
        weight_copy.start()
    fill_bias(table_ref, halo_bias, own_bias)
    own_codes = codes_of(packed_ref, rows, 2 * TILE - SEG)
    copy.wait()
    own_part(
        query_ref[...], packed_ref[0:rows, :], own_codes, own_bias, band, swapped, partial_ref, top_ref, total_ref
    )
    for weight_copy in weight_copies:
        weight_copy.wait()


def before_two_kernel(
    normed_ref, weight_ref, kv_weight_ref, packed_ref, table_ref, query_ref, halo_bias, partial_ref, top_ref, total_ref,
    own_bias, band, swapped,
):
    rows = normed_ref.shape[0]
    own = jnp.dot(normed_ref[...], kv_weight_ref[...], preferred_element_type=F32).astype(BF16)
    query = jnp.dot(normed_ref[...], weight_ref[...], preferred_element_type=F32).astype(BF16)
    query_ref[...] = query
    fill_bias(table_ref, halo_bias, own_bias)
    own_codes = codes_of(packed_ref, rows, 2 * TILE - SEG)
    own_part(query, own, own_codes, own_bias, band, swapped, partial_ref, top_ref, total_ref)


def with_residual(partial, residual):
    mine = (lax.axis_index("tp") == 0).astype(F32)
    wide = residual.astype(F32)
    half = wide.shape[1]
    return (partial[:, 0:half] + wide * mine).astype(BF16), (partial[:, half:] + wide * (1.0 - mine)).astype(BF16)


def near_one_kernel(
    query_ref, near_ref, packed_ref, halo_bias, partial_ref, top_ref, total_ref, weight_ref, residual_ref,
    out_ref, head_partial, head_top, head_total, head_left, head_code, band, swapped, mixed,
):
    rows = query_ref.shape[0]
    near_part(
        query_ref, near_ref[0:rows, :], codes_of(near_ref, rows, 0), codes_of(packed_ref, rows, 2 * TILE - SEG),
        halo_bias, partial_ref, top_ref, total_ref, band, swapped, mixed,
        (head_partial, head_top, head_total, head_left, head_code),
    )
    partial = jnp.dot(mixed[...], weight_ref[...], preferred_element_type=F32)
    half = residual_ref.shape[1]
    out_ref[:, 0:half], out_ref[:, half:] = with_residual(partial, residual_ref[SEG:, :])


def near_two_kernel(
    query_ref, near_ref, near_codes_ref, packed_ref, halo_bias, partial_ref, top_ref, total_ref, weight_ref,
    mine_ref, theirs_ref, head_partial, head_top, head_total, head_left, head_code, band, swapped, mixed,
):
    rows = query_ref.shape[0]
    near_part(
        query_ref, near_ref[...], codes_of(near_codes_ref, rows, 0), codes_of(packed_ref, rows, 2 * TILE - SEG),
        halo_bias, partial_ref, top_ref, total_ref, band, swapped, mixed,
        (head_partial, head_top, head_total, head_left, head_code),
    )
    half = mine_ref.shape[1]
    first = lax.axis_index("tp") == 0
    partial = jnp.dot(mixed[...], weight_ref[...], preferred_element_type=F32).astype(BF16)
    mine_ref[...] = jnp.where(first, partial[:, 0:half], partial[:, half:])
    theirs_ref[...] = jnp.where(first, partial[:, half:], partial[:, 0:half])


def far_one_kernel(
    far_ref, halo_bias, rest_ref, partial_ref, top_ref, total_ref, left_ref, code_ref, weight_ref, residual_ref,
    out_ref, mixed,
):
    out_ref[SEG:, :] = rest_ref[...]
    far_part(
        far_ref[0:SEG, :], codes_of(far_ref, SEG, 0), halo_bias, partial_ref, top_ref, total_ref, left_ref, code_ref, mixed
    )
    partial = jnp.dot(mixed[...], weight_ref[...], preferred_element_type=F32)
    half = residual_ref.shape[1]
    out_ref[0:SEG, 0:half], out_ref[0:SEG, half:] = with_residual(partial, residual_ref[0:SEG, :])


def far_two_kernel(
    far_ref, far_codes_ref, halo_bias, rest_theirs_ref, partial_ref, top_ref, total_ref, left_ref, code_ref, weight_ref,
    mine_ref, theirs_ref, mixed,
):
    half = mine_ref.shape[1]
    first = lax.axis_index("tp") == 0
    theirs_ref[SEG:, :] = rest_theirs_ref[...]
    far_part(
        far_ref[...], codes_of(far_codes_ref, SEG, 0), halo_bias, partial_ref, top_ref, total_ref, left_ref, code_ref, mixed
    )
    partial = jnp.dot(mixed[...], weight_ref[...], preferred_element_type=F32).astype(BF16)
    mine_ref[...] = jnp.where(first, partial[:, 0:half], partial[:, half:])
    theirs_ref[0:SEG, :] = jnp.where(first, partial[:, half:], partial[:, 0:half])


def norm_kernel(both_ref, gain_ref, other_weight_ref, send_ref, tail_ref, normed_ref, share_ref):
    layer = both_ref[0] + both_ref[1]
    wide = layer.astype(F32)
    rows, channels = wide.shape
    scale = lax.rsqrt(jnp.mean(wide * wide, axis=1, keepdims=True) + EPS)
    normed = (wide * scale * gain_ref[...]).astype(BF16)
    send = jnp.dot(normed, other_weight_ref[...], preferred_element_type=F32).astype(BF16)
    send_ref[...] = send
    tail_ref[...] = send[rows - SEG :]
    normed_ref[...] = normed
    half = channels // 2
    share_ref[...] = jnp.where(lax.axis_index("tp") == 0, layer[:, 0:half], layer[:, half:])


def last_kernel(both_ref, head_ref, rest_ref, share_ref, out_hbm, out, sems):
    first = lax.axis_index("tp") == 0
    copies = []
    parts = sems.shape[0]
    rows = SEG
    for part in range(parts):
        spot = slice(rows * part, rows * (part + 1))
        theirs = jnp.where(first, both_ref[1, spot, :], both_ref[0, spot, :])
        mine = rest_ref[spot.start - SEG : spot.stop - SEG, :] if part else head_ref[...]
        out[spot, :] = (
            share_ref[spot, :].astype(F32) + mine.astype(F32) + theirs.astype(F32)
        ).astype(BF16)
        copies.append(pltpu.make_async_copy(out.at[spot, :], out_hbm.at[spot, :], sems.at[part]))
        copies[-1].start()
    for copy in copies:
        copy.wait()


def call(kernel, outs, scratch, args, flops, mib=16, spaces=None, out_space=pltpu.VMEM):
    return pl.pallas_call(
        kernel,
        out_shape=outs,
        in_specs=[whole()] * len(args) if spaces is None else [pl.BlockSpec(memory_space=s) for s in spaces],
        out_specs=jax.tree.map(lambda _: pl.BlockSpec(memory_space=out_space), outs),
        scratch_shapes=scratch,
        compiler_params=params(mib),
        cost_estimate=cost(flops),
    )(*args)


def body(
    residual,
    query_first,
    key_first,
    value_first,
    documents,
    bias_first,
    out_first,
    norm_gain,
    query_w,
    key_w,
    value_w,
    bias_second,
    out_second,
):
    rows, half = residual.shape
    width = query_first.shape[1]
    channels = out_first.shape[1]
    docs = documents.reshape(1, rows)
    gain = norm_gain.reshape(1, channels)
    bands = [pltpu.VMEM((2 * TILE, 2 * TILE), BF16), pltpu.VMEM((2 * TILE, 2 * TILE), BF16)]
    before_scratch = [pltpu.VMEM((2, 4 * SEG, 3 * TILE), F32), *bands]
    near_scratch = [*bands, pltpu.VMEM((rows - SEG, width), BF16)]
    far_scratch = [pltpu.VMEM((SEG, width), BF16)]
    stats = shape(24 * SEG, TILE, dtype=F32)
    head_stats = shape(8 * SEG, TILE, dtype=F32)
    near_shapes = (
        shape(rows - SEG, channels),
        head_stats,
        head_stats,
        head_stats,
        shape(8 * SEG, TILE),
        shape(SEG, TILE, dtype=F32),
    )
    own_shapes = (shape(2, 2, 4 * SEG, 2 * TILE, dtype=F32), stats, stats, stats)
    packed, far_send = call(
        pack_kernel,
        (shape(rows + 8, 2 * TILE), shape(SEG + 8, 2 * TILE)),
        [pltpu.VMEM((8, 2 * TILE), F32), pltpu.VMEM((1, rows), jnp.int32), pltpu.SemaphoreType.DMA((7,))],
        tuple(pltpu.with_memory_space_constraint(x, pltpu.HBM) for x in (key_first, value_first, docs)),
        1 << 20,
        spaces=[pltpu.HBM] * 3,
    )
    near_one = from_behind(packed, 1)
    far_one = from_behind(far_send, 2)
    query_one, weights, *own_one = call(
        before_one_kernel,
        (shape(rows, width), shape(channels, 2 * TILE), *own_shapes),
        [*before_scratch, pltpu.SemaphoreType.DMA((3,))],
        (
            *(pltpu.with_memory_space_constraint(x, pltpu.HBM) for x in (query_first, key_w, value_w)),
            packed,
            bias_first,
        ),
        1 << 31,
        spaces=[pltpu.HBM] * 3 + [pltpu.VMEM] * 2,
    )
    other_weights = lax.ppermute(weights, "tp", [(0, 1), (1, 0)])
    rest_one = call(
        near_one_kernel,
        near_shapes,
        near_scratch,
        (query_one, near_one, packed, *own_one, out_first, residual),
        1 << 31,
    )
    sent_one = call(
        far_one_kernel,
        shape(rows, channels),
        far_scratch,
        (far_one, own_one[0], *rest_one, out_first, residual),
        1 << 31,
    )
    both_one = lax.all_gather(sent_one, "tp", axis=0)
    send_two, tail_two, normed, share = call(
        norm_kernel,
        (
            shape(rows, 2 * TILE),
            shape(SEG, 2 * TILE),
            shape(rows, channels),
            shape(rows, half),
        ),
        [],
        (both_one, gain, other_weights),
        1 << 30,
    )
    near_two = from_behind(send_two, 1, across=True)
    far_two = from_behind(tail_two, 2, across=True)
    query_two, *own_two = call(
        before_two_kernel,
        (shape(rows, width), *own_shapes),
        before_scratch,
        (normed, query_w, weights, packed, bias_second),
        1 << 31,
    )
    rest_mine, *rest_two = call(
        near_two_kernel,
        (shape(rows - SEG, half), shape(rows - SEG, half), *near_shapes[1:]),
        near_scratch,
        (query_two, near_two, near_one, packed, *own_two, out_second),
        1 << 31,
    )
    mine_two, sent_two = call(
        far_two_kernel,
        (shape(SEG, half), shape(rows, half)),
        far_scratch,
        (far_two, far_one, own_two[0], *rest_two, out_second),
        1 << 31,
    )
    both_two = lax.all_gather(sent_two, "tp", axis=0)
    return call(
        last_kernel,
        shape(rows, half),
        [pltpu.VMEM((rows, half), BF16), pltpu.SemaphoreType.DMA((3,))],
        (both_two, mine_two, rest_mine, share),
        1 << 20,
        out_space=pltpu.HBM,
    )


def solution(mesh):
    placed = (
        P("sp", "tp"),
        P("sp", "tp"),
        P("sp", "tp"),
        P("sp", "tp"),
        P("sp"),
        P("tp", None),
        P("tp", None),
        P(),
        P(None, "tp"),
        P(None, "tp"),
        P(None, "tp"),
        P("tp", None),
        P("tp", None),
    )
    return jax.shard_map(body, mesh=mesh, in_specs=placed, out_specs=P("sp", "tp"), check_vma=False)
```
